32 devices in a mesh: sp: 16 (over z, y, x), tp: 2 (over core).
Axes of the slice: x: 2, y: 2, z: 4, core: 2. Of those that a mesh axis runs over, the one named last changes fastest.
Arguments:
- query_rows: bfloat16 [4096, 1024], P('sp', 'tp'), may hold values from -6 to 6
- key_rows: bfloat16 [4096, 1024], P('sp', 'tp'), may hold values from -6 to 6
- value_rows: bfloat16 [4096, 1024], P('sp', 'tp'), may hold values from -6 to 6
- out_weight: bfloat16 [1024, 2048], P('tp'), may hold values from -0.75 to 0.75
Outputs:
- layer_out: bfloat16 [4096, 2048], P(('sp', 'tp'))
The draws below stay inside these ranges and needn't reach their ends.
All inputs are finite; a program needn't handle non-finite values.
Results may differ from the reference program's by a relative error of at most 0.012.
Values may be sent and summed in bfloat16 or wider, within the bound.
A program may use at most 64 MiB of HBM per device.

```python
import math
import jax
import jax.numpy as jnp
from jax import lax

D = 2048
H = 16
HD = 64
BACK = 128
SEQ = 4096


def planted_pair(key):
    base = jax.random.fold_in(key, 11)
    width = H * HD
    first = jnp.clip(jax.random.normal(jax.random.fold_in(base, 1), (SEQ, width), jnp.float32), -6.0, 6.0)
    second = jnp.clip(jax.random.normal(jax.random.fold_in(base, 2), (SEQ, width), jnp.float32), -6.0, 6.0)
    return (first, second)


def draw_query_rows(key, part):
    return planted_pair(key)[0].astype(jnp.bfloat16)


def draw_key_rows(key, part):
    return planted_pair(key)[1].astype(jnp.bfloat16)


def shard_levels(rng, dims, shards, smallest, high):
    factor_of, own = 1.0, jax.random.fold_in(rng, 6)
    for position, blocks in shards:
        heights = jnp.exp(jax.random.uniform(jax.random.fold_in(own, position), (blocks,), jnp.float32, smallest / len(shards), high / len(shards)))
        factor_of = factor_of * jnp.repeat(heights, dims[position] // blocks).reshape([-1 if axis == position else 1 for axis in range(len(dims))])
    return factor_of


def noise(rng, dims, scale, reach, pieces=(), kind=jnp.bfloat16):
    values = jax.random.normal(rng, dims, jnp.float32) * scale
    if len(pieces) > 0:
        values = shard_levels(rng, dims, pieces, -0.22, 0.18) * values
    return jnp.clip(values, min=-reach, max=reach).astype(kind)


def setup_inputs(seed: int = 0) -> dict:
    seeds = jax.random.split(jax.random.key(seed), 5)
    query_rows = draw_query_rows(jax.random.fold_in(seeds[4], 71), 0)
    key_rows = draw_key_rows(jax.random.fold_in(seeds[4], 71), 0)
    value_rows = noise(seeds[2], (SEQ, H * HD), 1.0, 6.0, ((0, 16), (1, 2)))
    out_weight = noise(seeds[3], (H * HD, D), HD ** -0.5, 0.75, ((0, 2),))
    return {"query_rows": query_rows, "key_rows": key_rows, "value_rows": value_rows, "out_weight": out_weight}


THETA = 500000.0
DILATIONS = (1, 4, 16)

def rotate(rows, positions, head_count, head_dim):
    half_dim = head_dim // 2
    inverse = jnp.power(jnp.float32(THETA), -jnp.arange(half_dim, dtype=jnp.float32) / half_dim)
    angles = positions.astype(jnp.float32)[:, None] * inverse[None, :]
    cosine = jnp.cos(angles)[:, None, :]
    sine = jnp.sin(angles)[:, None, :]
    whole = rows.astype(jnp.float32).reshape(rows.shape[0], head_count, head_dim)
    lower = whole[..., :half_dim]
    upper = whole[..., half_dim:]
    turned = jnp.concatenate([lower * cosine - upper * sine, upper * cosine + lower * sine], axis=-1)
    return turned.reshape(rows.shape[0], head_count * head_dim).astype(jnp.bfloat16)

def one_pattern(queries, key_seq, value_seq, dilation):
    head_dim = queries.shape[1]
    length = queries.shape[0] // dilation
    blocks = -(-length // BACK)
    padded = blocks * BACK

    def residue(rows):
        return rows.reshape(length, dilation, head_dim).transpose(1, 0, 2)
    query_sub = jnp.pad(residue(queries), ((0, 0), (0, padded - length), (0, 0)))
    query_sub = query_sub.reshape(dilation, blocks, BACK, head_dim)

    def with_prior(rows):
        extended = jnp.pad(residue(rows), ((0, 0), (BACK, padded - length), (0, 0)))
        prior = extended[:, :padded].reshape(dilation, blocks, BACK, head_dim)
        current = extended[:, BACK:].reshape(dilation, blocks, BACK, head_dim)
        return jnp.concatenate([prior, current], axis=2)
    key_sub = with_prior(key_seq)
    value_sub = with_prior(value_seq)
    scores = jnp.einsum('rnqc,rnkc->rnqk', query_sub.astype(jnp.float32), key_sub.astype(jnp.float32))
    scores = scores * (1.0 / math.sqrt(head_dim))
    query_index = jnp.arange(BACK)[:, None]
    key_index = jnp.arange(2 * BACK)[None, :]
    distance = query_index + BACK - key_index
    key_place = jnp.arange(blocks)[:, None, None] * BACK + key_index[None] - BACK
    allowed = (distance >= 0) & (distance <= BACK) & (key_place >= 0)
    scores = jnp.where(allowed[None], scores, -jnp.inf)
    row_max = lax.optimization_barrier(jnp.max(scores, axis=-1))
    weights = jnp.exp(scores - row_max[..., None])
    row_sum = lax.optimization_barrier(jnp.sum(weights, axis=-1))
    rounded = weights.astype(jnp.bfloat16)
    weighted = jnp.einsum('rnqk,rnkc->rnqc', rounded.astype(jnp.float32), value_sub.astype(jnp.float32))
    result = (weighted / row_sum[..., None]).astype(jnp.bfloat16)
    result = result.reshape(dilation, padded, head_dim)[:, :length].transpose(1, 0, 2)
    result = result.reshape(length * dilation, head_dim)
    row_max = row_max.reshape(dilation, padded)[:, :length].transpose(1, 0).reshape(-1)
    row_sum = row_sum.reshape(dilation, padded)[:, :length].transpose(1, 0).reshape(-1)
    return (result, row_max, row_sum)

def reference(query_rows, key_rows, value_rows, out_weight):
    positions = jnp.arange(SEQ, dtype=jnp.int32)
    turned_q = rotate(query_rows, positions, H, HD)
    turned_k = rotate(key_rows, positions, H, HD)

    def split(rows):
        return rows.reshape(SEQ, H, HD).transpose(1, 0, 2)

    def per_head(stacked):
        query_head, key_head, value_head = stacked
        results, maxima, sums = ([], [], [])
        for dilation in DILATIONS:
            result, row_max, row_sum = one_pattern(query_head, key_head, value_head, dilation)
            results.append(result)
            maxima.append(row_max)
            sums.append(row_sum)
        return (tuple(results), tuple(maxima), tuple(sums))
    results, maxima, sums = lax.map(per_head, (split(turned_q), split(turned_k), split(value_rows)))
    top = jnp.maximum(jnp.maximum(maxima[0], maxima[1]), maxima[2])
    scales = [sums[i] * jnp.exp(maxima[i] - top) for i in range(3)]
    weighted = scales[0][..., None] * results[0].astype(jnp.float32)
    weighted = weighted + scales[1][..., None] * results[1].astype(jnp.float32)
    weighted = weighted + scales[2][..., None] * results[2].astype(jnp.float32)
    denominator = scales[0] + scales[1] + scales[2]
    mixed = weighted / denominator[..., None]
    mixed = mixed.transpose(1, 0, 2).reshape(SEQ, H * HD).astype(jnp.bfloat16)
    return jnp.dot(mixed, out_weight, preferred_element_type=jnp.float32).astype(jnp.bfloat16)
```

```python
import functools
import math

import jax
import jax.numpy as jnp
import numpy as np
from jax import lax
from jax.experimental import pallas as pl
from jax.experimental.pallas import tpu as pltpu
from jax.sharding import PartitionSpec as P

HD = 64
BACK = 128
THETA = 500000.0
FAR = -1e30
F32 = jnp.float32
BF16 = jnp.bfloat16
LANES = 2 * HD
CHUNKS = 4
PIECE = BACK // CHUNKS
NT = (((1,), (1,)), ((), ()))


def place(p):
    return ((p & 7) << 4) + (((p >> 3) & 3) << 2) + (p >> 5)


def iota(shape, axis):
    return lax.broadcasted_iota(jnp.int32, shape, axis)


def kernel(
    G, ngroups, tp_count,
    q_hbm, k_hbm, v_hbm, cosb_hbm, sinb_hbm, inv_hbm, w_ref, out_ref,
    q_ref, k_ref, v_ref, cosb_ref, sinb_ref, inv_ref, qs, kvs, qr, kv, kvf, q2, q2f, acc, top,
    qb, qbf, accb, topb, ob, oin, b1_ref, b4_ref, b16_ref, wbuf, rs, rr, mx,
    s_kv, s_q, s_qb, s_x, s_o, s_ret, r_kv, r_q, r_qb, r_x, r_o, r_ret, w_sem, in_sem,
):
    loads = [
        pltpu.make_async_copy(source, dest, in_sem.at[n])
        for n, (source, dest) in enumerate((
            (inv_hbm, inv_ref), (cosb_hbm, cosb_ref), (sinb_hbm, sinb_ref),
            (k_hbm, k_ref), (v_hbm, v_ref), (q_hbm, q_ref),
        ))
    ]
    for load in loads:
        load.start()
    sp = lax.axis_index("sp")
    tp = lax.axis_index("tp")
    group = sp // G
    me = sp - group * G
    base = group * G
    has_prev = group > 0
    has_next = group < ngroups - 1
    seat = me * tp_count + tp
    seats = G * tp_count
    head = tp * G + me
    tok = q_ref.shape[0]
    halves = tok // BACK
    nq = G * halves
    own0 = 1

    def target(s, t):
        return {"sp": s, "tp": t}

    barrier = pltpu.get_barrier_semaphore()
    for o in range(1, seats):
        n = lax.rem(seat + o, seats)
        pl.semaphore_signal(
            barrier, inc=1, device_id=target(base + n // tp_count, lax.rem(n, tp_count)),
            device_id_type=pl.DeviceIdType.MESH,
        )

    @pl.when(has_prev)
    def _():
        for o in range(G):
            pl.semaphore_signal(
                barrier, inc=1, device_id=target(base - G + o, tp),
                device_id_type=pl.DeviceIdType.MESH,
            )

    @pl.when(has_next)
    def _():
        for o in range(G):
            pl.semaphore_signal(
                barrier, inc=1, device_id=target(base + G + o, tp),
                device_id_type=pl.DeviceIdType.MESH,
            )

    w_local = pltpu.make_async_copy(w_ref, wbuf.at[tp], w_sem.at[0])
    w_local.start()

    def stride4(n):
        w = n & 31
        return ((n >> 5) << 5) + ((w & 7) << 2) + (w >> 3)

    def masked(distance):
        return jnp.where((distance >= 0) & (distance <= BACK), 0.0, FAR)

    row = iota((BACK, 2 * BACK), 0)
    col = iota((BACK, 2 * BACK), 1)
    b1_ref[...] = masked(place(row) + BACK - place(col & (BACK - 1)) - ((col >> 7) << 7))
    b4_ref[...] = masked(stride4(row) + BACK - stride4(col))
    b16_ref[...] = masked(row + BACK - col)

    scope = jax.named_scope
    with scope("a_loads"):
        for load in loads:
            load.wait()

    lane = iota((BACK, LANES), 1)
    low = lane < HD
    lane_t = iota((tok, LANES), 1)
    first = (lane_t & (HD - 1)) < HD // 2
    angle = inv_ref[...] * (sp * tok).astype(F32)
    ca = jnp.cos(angle)[:1]
    sa = jnp.sin(angle)[:1]
    cos = ca * cosb_ref[...] - sa * sinb_ref[...]
    sin = sa * cosb_ref[...] + ca * sinb_ref[...]
    sin = jnp.where(first, -sin, sin)
    swizzle = jnp.where(place(iota((BACK, BACK), 0)) == iota((BACK, BACK), 1), 1.0, 0.0).astype(BF16)
    back = jnp.where(place(iota((BACK, BACK), 1)) == iota((BACK, BACK), 0), 1.0, 0.0).astype(BF16)

    def turn(ref, cols):
        x = ref[:, cols].astype(F32)
        other = jnp.where(first, pltpu.roll(x, LANES - HD // 2, 1), pltpu.roll(x, HD // 2, 1))
        return (x * cos + other * sin).astype(BF16)

    def sw(x):
        return jnp.dot(swizzle, x, preferred_element_type=F32)

    def cut(x):
        return x.astype(BF16).reshape(CHUNKS, PIECE, LANES)

    with scope("c_turn"):
        for m in range(G // 2):
            cols = slice(m * LANES, (m + 1) * LANES)
            tq = turn(q_ref, cols)
            tk = turn(k_ref, cols)
            tv = v_ref[:, cols]
            q_a = sw(tq[:BACK]) * (1.0 / math.sqrt(HD))
            q_b = sw(tq[BACK:]) * (1.0 / math.sqrt(HD))
            qs[:, 2 * m] = cut(jnp.where(low, q_a, pltpu.roll(q_b, HD, 1)))
            qs[:, 2 * m + 1] = cut(jnp.where(low, pltpu.roll(q_a, HD, 1), q_b))
            for e in range(halves):
                ks = sw(tk[e * BACK : (e + 1) * BACK])
                vs = sw(tv[e * BACK : (e + 1) * BACK])
                kvs[:, 2 * m, e] = cut(jnp.where(low, ks, pltpu.roll(vs, HD, 1)))
                kvs[:, 2 * m + 1, e] = cut(jnp.where(low, pltpu.roll(ks, HD, 1), vs))

    with scope("d_barrier"):
        pl.semaphore_wait(
            barrier, seats - 1 + jnp.where(has_prev, G, 0) + jnp.where(has_next, G, 0)
        )

    def remote(source, dest, send, recv, device):
        return pltpu.make_async_remote_copy(
            src_ref=source, dst_ref=dest, send_sem=send, recv_sem=recv,
            device_id=device, device_id_type=pl.DeviceIdType.MESH,
        )

    def drain(ref, sem):
        pltpu.make_async_copy(ref, ref, sem).wait()

    def copy_kv(c, dest):
        return remote(
            kvs.at[c, dest], kv.at[c, pl.ds(own0 + halves * me, halves)],
            s_kv, r_kv.at[c], target(base + dest, tp),
        )

    def copy_q(c, dest):
        return remote(qs.at[c, dest], qr.at[c, me], s_q, r_q.at[c], target(base + dest, tp))

    def copy_qb(c, dest):
        return remote(
            qs.at[c, dest], qb.at[c, me], s_qb, r_qb.at[c], target(base - G + dest, tp)
        )

    w_away = pltpu.make_async_remote_copy(
        src_ref=w_ref, dst_ref=wbuf.at[tp], send_sem=w_sem.at[1], recv_sem=w_sem.at[2],
        device_id=target(sp, tp_count - 1 - tp), device_id_type=pl.DeviceIdType.MESH,
    )

    bits = [1 << n for n in range(G.bit_length() - 1)]
    far = sorted(range(1, G), key=lambda o: -o.bit_count())

    def mate(o):
        return sum((((me // b + o // b) % 2) * b for b in bits), 0)

    with scope("e_issue"):
        for c in range(CHUNKS):
            @pl.when(has_prev)
            def _():
                for o in [*far, 0]:
                    copy_qb(c, mate(o)).start()

            for o in far:
                copy_q(c, mate(o)).start()
                copy_kv(c, mate(o)).start()

        w_away.start()

    for c in range(CHUNKS):
        kv[c, pl.ds(own0 + halves * me, halves)] = kvs[c, me]
        qr[c, me] = qs[c, me]

    low_p = low[:PIECE]

    def unpack(ref, c, wide, narrow=None):
        for s in range(G):
            x = ref[c, s].astype(F32)
            a = jnp.where(low_p, x, 0.0)
            b = jnp.where(low_p, pltpu.roll(x, HD, 1), 0.0)
            wide[2 * s] = a
            wide[2 * s + 1] = b
            if narrow is not None:
                narrow[c, 2 * s] = a.astype(BF16)
                narrow[c, 2 * s + 1] = b.astype(BF16)

    def run(tiles, fresh=False, sums=acc, tops=top):
        done = []
        for q, keys, b, ref_at in tiles:
            s = lax.dot_general(q, keys, NT, preferred_element_type=F32) + b
            t = jnp.max(s, axis=1, keepdims=True)
            shape = sums[ref_at].shape
            if fresh:
                t = jnp.broadcast_to(t, (q.shape[0], LANES))
            else:
                t_old = tops[ref_at].reshape(-1, LANES)
                t = jnp.maximum(t_old, t)
            p = jnp.concatenate(
                [jnp.exp(s[:, n : n + LANES] - t) for n in range(0, s.shape[1], LANES)], axis=1
            ).astype(BF16)
            ones = jnp.where(iota(keys.shape, 1) < HD, jnp.ones_like(keys), keys)
            o = jnp.dot(p, ones, preferred_element_type=F32)
            if not fresh:
                o = sums[ref_at].reshape(-1, LANES) * jnp.exp(t_old - t) + o
            done.append((ref_at, o.reshape(shape), t.reshape(shape)))
        for ref_at, o, t in done:
            sums[ref_at] = o
            tops[ref_at] = t

    every = slice(None)

    def block(h):
        return kv[:, own0 + h].reshape(BACK, LANES)

    def tile1(h):
        return (
            q2[:, h].reshape(BACK, LANES), jnp.concatenate([block(h - 1), block(h)], axis=0),
            b1_ref[...], (every, h),
        )

    def tile1_part(e):
        return (
            q2[:, 0].reshape(BACK, LANES), block(e - 1),
            b1_ref[:, e * BACK : (e + 1) * BACK], (every, 0),
        )

    def tile4(c, n):
        blocks = slice(4 * n, 4 * n + 4)
        return (
            q2[c, blocks].reshape(BACK, LANES),
            kv[c, own0 + 4 * n - 4 : own0 + 4 * n + 4].reshape(2 * BACK, LANES),
            b4_ref[...], (c, blocks),
        )

    def tile4_new(c):
        return (
            q2[c, :4].reshape(BACK, LANES), kv[c, own0 : own0 + 4].reshape(BACK, LANES),
            b4_ref[:, BACK:], (c, slice(0, 4)),
        )

    def tile4_old(c):
        return (
            qbf[:4].reshape(BACK, LANES).astype(BF16),
            kv[c, own0 + nq - 4 : own0 + nq].reshape(BACK, LANES),
            b4_ref[:, :BACK], (slice(0, 4),),
        )

    def tile16(i, queries, e, ref_at):
        rows = slice(8 * i, 8 * i + 8)
        return (
            queries[:, rows].reshape(BACK, LANES).astype(BF16),
            kvf[:, rows].reshape(BACK, LANES).astype(BF16),
            b16_ref[:, e * BACK : (e + 1) * BACK], (*ref_at, every, rows),
        )

    each = range(PIECE // 8)
    half = PIECE // 2
    eight = BACK // half
    lane_h = iota((eight, half, LANES), 2)
    low_h = lane_h < HD
    flat = (BACK, LANES)

    def rounded(x):
        return x.astype(BF16).astype(F32)

    def send_old(c):
        stats = jnp.zeros((2 * 8, LANES), F32)
        for g in range(nq // eight):
            at = slice(g * eight, (g + 1) * eight)
            t = topb[at]
            mark = rounded(t)
            a = accb[at] * jnp.exp(t - mark)
            z = pltpu.roll(a, HD, 2)
            lo, hi = a[:, :half], a[:, half:]
            ob[c, g * BACK : (g + 1) * BACK] = (
                jnp.where(low_h, z[:, :half], hi).astype(BF16).reshape(flat)
            )
            columns = mark[:, half:]
            columns = jnp.where(lane_h == 0, mark[:, :half], columns)
            columns = jnp.where(lane_h == 2, rounded(lo), columns)
            columns = jnp.where(lane_h == 3, rounded(hi), columns)
            columns = jnp.where(lane_h == 4, lo - rounded(lo), columns)
            columns = jnp.where(lane_h == 5, hi - rounded(hi), columns)
            pick = (iota((2 * 8, LANES), 0) - 8 * g == iota((2 * 8, LANES), 1)) & (
                iota((2 * 8, LANES), 1) < 6
            )
            stats = stats + lax.dot_general(
                jnp.where(pick, 1.0, 0.0).astype(BF16), columns.astype(BF16).reshape(flat), NT,
                preferred_element_type=F32,
            )
        ob[c, nq * half :] = stats.astype(BF16)
        copy_o(c).start()

    def copy_o(c):
        return remote(ob.at[c], oin.at[c], s_o, r_o.at[c], target(sp + G, tp))

    def copy_x():
        return remote(kv.at[:, own0 + nq - 1], kv.at[:, 0], s_x, r_x, target(sp + G, tp))

    with scope("h_chunks"):
        @pl.loop(0, CHUNKS)
        def _(c):
            drain(qr.at[c, : G - 1], r_q.at[c])
            drain(kv.at[c, own0 : own0 + halves * (G - 1)], r_kv.at[c])
            kvf[...] = kv[c, own0:].astype(F32)

            @pl.when(has_next)
            def _():
                drain(qb.at[c], r_qb.at[c])
                unpack(qb, c, qbf)
                run([tile16(i, qbf, 0, ()) for i in each], True, accb, topb)
                run([tile4_old(c)], False, accb, topb)
                send_old(c)

            unpack(qr, c, q2f, q2)
            run([tile4_new(c)] + [tile4(c, n) for n in range(1, nq // 4)], True)
            run([tile16(i, q2f, 1, (c,)) for i in each])

    with scope("i_t1"):
        @pl.when(has_next)
        def _():
            copy_x().start()

        run([tile1_part(1)])

        @pl.loop(0, (nq - 1) // 5)
        def _(i):
            run([tile1(1 + 5 * i + n) for n in range(5)])

        @pl.when(has_prev)
        def _():
            drain(kv.at[:, 0], r_x)
            run([tile1_part(0)])

    eye = jnp.where(iota(flat, 0) == iota(flat, 1), 1.0, 0.0).astype(BF16)
    upper = iota(flat, 0) < HD

    def finish(c, merge):
        if merge:
            stats = oin[c, nq * half :].astype(F32)
        for g in range(nq // eight):
            at = slice(g * eight, (g + 1) * eight)
            a = acc[c, at]
            z = pltpu.roll(a, HD, 2)
            num = jnp.where(low_h, z[:, :half], a[:, half:]).reshape(flat)
            den = jnp.where(low_h, a[:, :half], z[:, half:]).reshape(flat)
            if merge:
                def spread(j):
                    both = jnp.where(
                        upper,
                        jnp.broadcast_to(stats[8 * g + j : 8 * g + j + 1], flat),
                        jnp.broadcast_to(stats[8 * g + j + 1 : 8 * g + j + 2], flat),
                    )
                    return lax.dot_general(eye, both.astype(BF16), NT, preferred_element_type=F32)

                t = top[c, at]
                t = jnp.where(low_h, t[:, :half], t[:, half:]).reshape(flat)
                t_old = spread(0)
                t_new = jnp.maximum(t, t_old)
                mine = jnp.exp(t - t_new)
                theirs = jnp.exp(t_old - t_new)
                num = num * mine + oin[c, g * BACK : (g + 1) * BACK].astype(F32) * theirs
                den = den * mine + (spread(2) + spread(4)) * theirs
            rs[c, at] = (num / den).astype(BF16).reshape(eight, half, LANES)

    def copy_ret(c, n):
        return remote(
            rs.at[c, n], rr.at[c, head], s_ret, r_ret,
            target(base + n // tp_count, lax.rem(n, tp_count)),
        )

    with scope("o_finish"):
        @pl.loop(0, CHUNKS)
        def _(c):
            @pl.when(has_prev)
            def _():
                drain(oin.at[c], r_o.at[c])
                finish(c, True)

            @pl.when(jnp.logical_not(has_prev))
            def _():
                finish(c, False)

            for o in far + [0]:
                copy_ret(c, mate(o) * tp_count + tp_count - 1 - tp).start()
                if o:
                    copy_ret(c, mate(o) * tp_count + tp).start()
            rr[c, head] = rs[c, seat]

    with scope("q_sendwait"):
        drain(kvs.at[:, : G - 1], s_kv)
        drain(qs.at[:, : G - 1], s_q)

        @pl.when(has_prev)
        def _():
            drain(qs, s_qb)

        @pl.when(has_next)
        def _():
            drain(ob, s_o)
            drain(kv.at[:, 0], s_x)

        w_local.wait()
        w_away.wait_send()
        pltpu.make_async_remote_copy(
            src_ref=w_ref, dst_ref=wbuf.at[tp_count - 1 - tp],
            send_sem=w_sem.at[1], recv_sem=w_sem.at[2],
            device_id=target(sp, tp_count - 1 - tp), device_id_type=pl.DeviceIdType.MESH,
        ).wait_recv()

    with scope("s_retwait"):
        drain(rr.at[:, : seats - 1], r_ret)

    low_s = iota((half, LANES), 1) < HD
    with scope("t_mix"):
        for m in range(seats // 2):
            x0 = rr[:, 2 * m].astype(F32)
            x1 = rr[:, 2 * m + 1].astype(F32)
            y0 = pltpu.roll(x0, HD, 2)
            y1 = pltpu.roll(x1, HD, 2)
            pair = jnp.concatenate(
                [jnp.where(low_s[None], x0, y1), jnp.where(low_s[None], y0, x1)], axis=1
            ).astype(BF16).reshape(BACK, LANES)
            mx[:, m * LANES : (m + 1) * LANES] = jnp.dot(
                back, pair, preferred_element_type=F32
            ).astype(BF16)

    width = wbuf.shape[1]
    step = 512

    with scope("u_proj"):
        @pl.loop(0, out_ref.shape[1] // step)
        def _(c):
            cols = pl.ds(pl.multiple_of(c * step, step), step)
            total = jnp.dot(mx[:, :width], wbuf[0, :, cols], preferred_element_type=F32)
            total = total + jnp.dot(mx[:, width:], wbuf[1, :, cols], preferred_element_type=F32)
            out_ref[:, cols] = total.astype(BF16)

    with scope("v_end"):
        drain(rs.at[:, : seats - 1], s_ret)


def per_device(sp_count, tp_count, query_rows, key_rows, value_rows, out_weight):
    tok = query_rows.shape[0]
    G = query_rows.shape[1] // HD
    halves = tok // BACK
    ngroups = sp_count // G
    assert tok == 2 * BACK and tp_count == 2 and sp_count % G == 0
    assert G & (G - 1) == 0
    assert G * tok == 16 * BACK
    inverse = np.power(THETA, -np.arange(HD // 2) / (HD // 2))
    inverse = np.tile(inverse, LANES // (HD // 2))[None, :]
    local = np.arange(tok)[:, None] * inverse
    cosb = jnp.asarray(np.cos(local), F32)
    sinb = jnp.asarray(np.sin(local), F32)
    inv = jnp.asarray(np.tile(inverse, (8, 1)), F32)
    seats = G * tp_count
    nq = G * halves
    vmem = pl.BlockSpec(memory_space=pltpu.VMEM)
    dma = pltpu.SemaphoreType.DMA
    return pl.pallas_call(
        functools.partial(kernel, G, ngroups, tp_count),
        out_shape=pltpu.VMEM((tok // tp_count, out_weight.shape[1]), BF16),
        in_specs=[pl.BlockSpec(memory_space=pl.ANY)] * 7,
        out_specs=vmem,
        scratch_shapes=[
            pltpu.VMEM(query_rows.shape, BF16),
            pltpu.VMEM(query_rows.shape, BF16),
            pltpu.VMEM(query_rows.shape, BF16),
            pltpu.VMEM(cosb.shape, F32),
            pltpu.VMEM(sinb.shape, F32),
            pltpu.VMEM(inv.shape, F32),
            pltpu.VMEM((CHUNKS, G, PIECE, LANES), BF16),
            pltpu.VMEM((CHUNKS, G, halves, PIECE, LANES), BF16),
            pltpu.VMEM((CHUNKS, G, PIECE, LANES), BF16),
            pltpu.VMEM((CHUNKS, 1 + nq, PIECE, LANES), BF16),
            pltpu.VMEM((nq, PIECE, LANES), F32),
            pltpu.VMEM((CHUNKS, nq, PIECE, LANES), BF16),
            pltpu.VMEM((nq, PIECE, LANES), F32),
            pltpu.VMEM((CHUNKS, nq, PIECE, LANES), F32),
            pltpu.VMEM((CHUNKS, nq, PIECE, LANES), F32),
            pltpu.VMEM((CHUNKS, G, PIECE, LANES), BF16),
            pltpu.VMEM((nq, PIECE, LANES), F32),
            pltpu.VMEM((nq, PIECE, LANES), F32),
            pltpu.VMEM((nq, PIECE, LANES), F32),
            pltpu.VMEM((CHUNKS, nq * PIECE // 2 + 16, LANES), BF16),
            pltpu.VMEM((CHUNKS, nq * PIECE // 2 + 16, LANES), BF16),
            pltpu.VMEM((BACK, 2 * BACK), F32),
            pltpu.VMEM((BACK, 2 * BACK), F32),
            pltpu.VMEM((BACK, 2 * BACK), F32),
            pltpu.VMEM((tp_count,) + out_weight.shape, BF16),
            pltpu.VMEM((CHUNKS, seats, PIECE // 2, LANES), BF16),
            pltpu.VMEM((CHUNKS, seats, PIECE // 2, LANES), BF16),
            pltpu.VMEM((BACK, seats * HD), BF16),
            dma, dma, dma, dma, dma, dma,
            dma((CHUNKS,)), dma((CHUNKS,)), dma((CHUNKS,)), dma, dma((CHUNKS,)), dma,
            dma((3,)), dma((6,)),
        ],
        compiler_params=pltpu.CompilerParams(
            collective_id=0, has_side_effects=True, vmem_limit_bytes=63 * 1024 * 1024
        ),
    )(query_rows, key_rows, value_rows, cosb, sinb, inv, out_weight)


def solution(mesh):
    return jax.shard_map(
        functools.partial(per_device, mesh.shape["sp"], mesh.shape["tp"]),
        mesh=mesh,
        in_specs=(P("sp", "tp"), P("sp", "tp"), P("sp", "tp"), P("tp", None)),
        out_specs=P(("sp", "tp"), None),
        check_vma=False,
    )
```

```python
import functools
import math

import jax
import jax.numpy as jnp
import numpy as np
from jax import lax
from jax.experimental import pallas as pl
from jax.experimental.pallas import tpu as pltpu
from jax.sharding import PartitionSpec as P

HD = 64
BACK = 128
THETA = 500000.0
FAR = -1e30
F32 = jnp.float32
BF16 = jnp.bfloat16
LANES = 2 * HD
CHUNKS = 4
PIECE = BACK // CHUNKS
NT = (((1,), (1,)), ((), ()))


def place(p):
    return ((p & 7) << 4) + (((p >> 3) & 3) << 2) + (p >> 5)


def iota(shape, axis):
    return lax.broadcasted_iota(jnp.int32, shape, axis)


def kernel(
    G, ngroups, tp_count,
    q_hbm, k_hbm, v_hbm, cosb_hbm, sinb_hbm, inv_hbm, w_ref, out_ref,
    q_ref, k_ref, v_ref, cosb_ref, sinb_ref, inv_ref, qs, kvs, qr, kv, kvf, q2, q2f,
    acc1, top1, acc4, top4, acc16, top16, accx, topx, qb, qbf, accb, topb, accb4, topb4, ob, oin, pn, pd, pt, b1_ref, b4_ref, b16_ref, bx_ref, wbuf, rs, rr, mx,
    s_kv, s_q, s_qb, s_x, s_o, s_ret, r_kv, r_q, r_qb, r_x, r_o, r_ret, w_sem, in_sem,
):
    loads = [
        pltpu.make_async_copy(source, dest, in_sem.at[n])
        for n, (source, dest) in enumerate((
            (inv_hbm, inv_ref), (cosb_hbm, cosb_ref), (sinb_hbm, sinb_ref),
            (k_hbm, k_ref), (v_hbm, v_ref), (q_hbm, q_ref),
        ))
    ]
    for load in loads:
        load.start()
    sp = lax.axis_index("sp")
    tp = lax.axis_index("tp")
    group = sp // G
    me = sp - group * G
    base = group * G
    has_prev = group > 0
    has_next = group < ngroups - 1
    seat = me * tp_count + tp
    seats = G * tp_count
    head = tp * G + me
    tok = q_ref.shape[0]
    halves = tok // BACK
    nq = G * halves
    hb = G // 2
    nh = nq // 2
    own0 = nh

    def target(s, t):
        return {"sp": s, "tp": t}

    barrier = pltpu.get_barrier_semaphore()
    for o in range(1, seats):
        n = lax.rem(seat + o, seats)
        pl.semaphore_signal(
            barrier, inc=1, device_id=target(base + n // tp_count, lax.rem(n, tp_count)),
            device_id_type=pl.DeviceIdType.MESH,
        )

    @pl.when(has_prev)
    def _():
        for o in range(G):
            pl.semaphore_signal(
                barrier, inc=1, device_id=target(base - G + o, tp),
                device_id_type=pl.DeviceIdType.MESH,
            )

    @pl.when(has_next)
    def _():
        for o in range(G):
            pl.semaphore_signal(
                barrier, inc=1, device_id=target(base + G + o, tp),
                device_id_type=pl.DeviceIdType.MESH,
            )

    w_local = pltpu.make_async_copy(w_ref, wbuf.at[tp], w_sem.at[0])
    w_local.start()

    def stride4(n):
        w = n & 31
        return ((n >> 5) << 5) + ((w & 7) << 2) + (w >> 3)

    def masked(distance):
        return jnp.where((distance >= 0) & (distance <= BACK), 0.0, FAR)

    row = iota((BACK, 2 * BACK), 0)
    col = iota((BACK, 2 * BACK), 1)
    b1_ref[...] = masked(place(row) + BACK - place(col & (BACK - 1)) - ((col >> 7) << 7))
    b4_ref[...] = masked(stride4(row) + BACK - stride4(col))
    b16_ref[...] = masked(row + BACK - col)

    def stride16(n):
        return ((n >> 4) << 3) + (n & 7)

    xrow = iota((BACK, BACK), 0)
    xcol = iota((BACK, BACK), 1)
    same = ((xrow ^ xcol) & 8) == 0
    bx_ref[...] = jnp.where(same, masked(stride16(xrow) + BACK - stride16(xcol)), FAR)

    scope = jax.named_scope
    with scope("a_loads"):
        for load in loads:
            load.wait()

    lane = iota((BACK, LANES), 1)
    low = lane < HD
    lane_t = iota((tok, LANES), 1)
    first = (lane_t & (HD - 1)) < HD // 2
    angle = inv_ref[...] * (sp * tok).astype(F32)
    ca = jnp.cos(angle)[:1]
    sa = jnp.sin(angle)[:1]
    cos = ca * cosb_ref[...] - sa * sinb_ref[...]
    sin = sa * cosb_ref[...] + ca * sinb_ref[...]
    sin = jnp.where(first, -sin, sin)
    swizzle = jnp.where(place(iota((BACK, BACK), 0)) == iota((BACK, BACK), 1), 1.0, 0.0).astype(BF16)
    back = jnp.where(place(iota((BACK, BACK), 1)) == iota((BACK, BACK), 0), 1.0, 0.0).astype(BF16)

    def turn(ref, cols):
        x = ref[:, cols].astype(F32)
        other = jnp.where(first, pltpu.roll(x, LANES - HD // 2, 1), pltpu.roll(x, HD // 2, 1))
        return (x * cos + other * sin).astype(BF16)

    def sw(x):
        return jnp.dot(swizzle, x, preferred_element_type=F32)

    def cut(x):
        return x.astype(BF16).reshape(CHUNKS, PIECE, LANES)

    with scope("c_turn"):
        for m in range(G // 2):
            cols = slice(m * LANES, (m + 1) * LANES)
            tq = turn(q_ref, cols)
            tk = turn(k_ref, cols)
            tv = v_ref[:, cols]
            q_a = sw(tq[:BACK]) * (1.0 / math.sqrt(HD))
            q_b = sw(tq[BACK:]) * (1.0 / math.sqrt(HD))
            qs[:, 2 * m] = cut(jnp.where(low, q_a, pltpu.roll(q_b, HD, 1)))
            qs[:, 2 * m + 1] = cut(jnp.where(low, pltpu.roll(q_a, HD, 1), q_b))
            for e in range(halves):
                ks = sw(tk[e * BACK : (e + 1) * BACK])
                vs = sw(tv[e * BACK : (e + 1) * BACK])
                kvs[:, 2 * m, e] = cut(jnp.where(low, ks, pltpu.roll(vs, HD, 1)))
                kvs[:, 2 * m + 1, e] = cut(jnp.where(low, pltpu.roll(ks, HD, 1), vs))

    with scope("d_barrier"):
        pl.semaphore_wait(
            barrier, seats - 1 + jnp.where(has_prev, G, 0) + jnp.where(has_next, G, 0)
        )

    def remote(source, dest, send, recv, device):
        return pltpu.make_async_remote_copy(
            src_ref=source, dst_ref=dest, send_sem=send, recv_sem=recv,
            device_id=device, device_id_type=pl.DeviceIdType.MESH,
        )

    def drain(ref, sem):
        pltpu.make_async_copy(ref, ref, sem).wait()

    def copy_kv(c, dest):
        return remote(
            kvs.at[c, dest], kv.at[c, pl.ds(own0 + halves * me, halves)],
            s_kv, r_kv.at[c], target(base + dest, tp),
        )

    def copy_q(c, dest):
        return remote(qs.at[c, dest], qr.at[c, me], s_q, r_q.at[c], target(base + dest, tp))

    def copy_qb(c, dest):
        return remote(
            qs.at[c, dest], qb.at[c, me], s_qb, r_qb.at[c], target(base - G + dest, tp)
        )

    def copy_x(c, dest):
        return remote(
            kvs.at[c, dest], kv.at[c, pl.ds(halves * (me - hb), halves)],
            s_x, r_x, target(base + G + dest, tp),
        )

    w_away = pltpu.make_async_remote_copy(
        src_ref=w_ref, dst_ref=wbuf.at[tp], send_sem=w_sem.at[1], recv_sem=w_sem.at[2],
        device_id=target(sp, tp_count - 1 - tp), device_id_type=pl.DeviceIdType.MESH,
    )

    bits = [1 << n for n in range(G.bit_length() - 1)]
    far = sorted(range(1, G), key=lambda o: -o.bit_count())

    quad = [o for o in far if o < hb] + [0]

    def mate(o):
        return sum((((me // b + o // b) % 2) * b for b in bits), 0)

    with scope("e_issue"):
        @pl.when(jnp.logical_and(has_next, me >= hb))
        def _():
            for part in (0, hb):
                for c in range(CHUNKS):
                    for o in quad:
                        copy_x(c, part + lax.rem(mate(o), hb)).start()

        for c in range(CHUNKS):
            @pl.when(jnp.logical_and(has_prev, me < hb))
            def _():
                for o in [*far, 0]:
                    copy_qb(c, mate(o)).start()

            for o in far:
                copy_q(c, mate(o)).start()
                copy_kv(c, mate(o)).start()

    for c in range(CHUNKS):
        kv[c, pl.ds(own0 + halves * me, halves)] = kvs[c, me]
        qr[c, me] = qs[c, me]

    low_p = low[:PIECE]

    def unpack(ref, c, wide, narrow=None):
        for s in range(ref.shape[1]):
            x = ref[c, s].astype(F32)
            a = jnp.where(low_p, x, 0.0)
            b = jnp.where(low_p, pltpu.roll(x, HD, 1), 0.0)
            wide[2 * s] = a
            wide[2 * s + 1] = b
            if narrow is not None:
                narrow[c, 2 * s] = a.astype(BF16)
                narrow[c, 2 * s + 1] = b.astype(BF16)

    def run(tiles):
        done = []
        for tile in tiles:
            q = jnp.concatenate([part[0] for part in tile], axis=0)
            keys = jnp.concatenate([part[1] for part in tile], axis=0)
            s = lax.dot_general(q, keys, NT, preferred_element_type=F32)
            rows, cols, ps, ts = 0, 0, [], []
            for part in tile:
                n, k = part[0].shape[0], part[1].shape[0]
                mine = s[rows : rows + n, cols : cols + k] + part[2]
                t = jnp.max(mine, axis=1, keepdims=True)
                p = [
                    jnp.exp(mine[:, a : a + LANES] - t).astype(BF16) for a in range(0, k, LANES)
                ]
                none = jnp.zeros_like(p[0])
                before, after = cols // LANES, (keys.shape[0] - cols - k) // LANES
                ps.append(jnp.concatenate([none] * before + p + [none] * after, axis=1))
                ts.append(t)
                rows, cols = rows + n, cols + k
            ones = jnp.where(iota(keys.shape, 1) < HD, jnp.ones_like(keys), keys)
            o = jnp.dot(jnp.concatenate(ps, axis=0), ones, preferred_element_type=F32)
            rows = 0
            for part, t in zip(tile, ts):
                end = rows + part[0].shape[0]
                done.append((part[3], o[rows:end], jnp.broadcast_to(t, (end - rows, LANES))))
                rows = end
        for places, o, t in done:
            first_row = 0
            for sums, tops, at in places:
                shape = sums[at].shape
                rows = slice(first_row, first_row + math.prod(shape[:-1]))
                sums[at] = o[rows].reshape(shape)
                tops[at] = t[rows].reshape(shape)
                first_row = rows.stop

    def pairs(tiles):
        return [tiles[n : n + 2] for n in range(0, len(tiles), 2)]

    every = slice(None)

    def block(h):
        return kv[:, own0 + h].reshape(BACK, LANES)

    def tile1(h):
        return (
            q2[:, h].reshape(BACK, LANES), jnp.concatenate([block(h - 1), block(h)], axis=0),
            jnp.where(missing, FAR, b1_ref[...]) if h == 0 else b1_ref[...],
            ((acc1, top1, (every, h)),),
        )

    def tile4(c, n):
        blocks = slice(4 * n, 4 * n + 4)
        return (
            q2[c, blocks].reshape(BACK, LANES),
            kv[c, own0 + 4 * n - 4 : own0 + 4 * n + 4].reshape(2 * BACK, LANES),
            b4_ref[...], ((acc4, top4, (c, blocks)),),
        )

    def tile4_first(c, alone):
        keys = kv[c, own0 : own0 + 4].reshape(BACK, LANES)
        b = b4_ref[:, BACK:]
        if alone:
            keys = jnp.concatenate([keys, keys], axis=0)
            b = jnp.concatenate([jnp.full_like(b, FAR), b], axis=1)
        return (q2[c, :4].reshape(BACK, LANES), keys, b, ((acc4, top4, (c, slice(0, 4))),))

    def tile4_old(c):
        return (
            qbf[:4].reshape(BACK, LANES).astype(BF16),
            kv[c, own0 + nq - 4 : own0 + nq].reshape(BACK, LANES),
            b4_ref[:, :BACK], ((accb4, topb4, (every,)),),
        )

    def tile16(c, i, both):
        rows = slice(8 * i, 8 * i + 8)
        q = q2f[c, :, rows].reshape(BACK, LANES).astype(BF16)
        b = b16_ref[:, BACK:]
        places = ((acc16, top16, (c, every, rows)),)
        if both:
            old = qbf[:, rows].reshape(-1, LANES).astype(BF16)
            q = jnp.concatenate([q, old], axis=0)
            b = jnp.concatenate([b, b16_ref[: old.shape[0], :BACK]], axis=0)
            places = (*places, (accb, topb, (every, rows)))
        return (q, kvf[:, rows].reshape(BACK, LANES).astype(BF16), b, places)

    def tilex(c, i):
        rows = slice(16 * i, 16 * i + 16)
        return (
            q2[c, nh:, rows].reshape(BACK, LANES), kv[c, :nh, rows].reshape(BACK, LANES),
            bx_ref[...], ((accx, topx, (c, every, rows)),),
        )

    each = range(PIECE // 8)
    half = PIECE // 2
    eight = BACK // half
    lane_h = iota((eight, half, LANES), 2)
    low_h = lane_h < HD
    flat = (BACK, LANES)

    def rounded(x):
        return x.astype(BF16).astype(F32)

    def send_old(c):
        t4, t16 = topb4[...], topb[:4]
        t = jnp.maximum(t4, t16)
        accb[:4] = accb[:4] * jnp.exp(t16 - t) + accb4[...] * jnp.exp(t4 - t)
        topb[:4] = t
        stats = jnp.zeros((2 * 8, LANES), F32)
        for g in range(1):
            at = slice(g * eight, (g + 1) * eight)
            t = topb[at]
            mark = rounded(t)
            a = accb[at] * jnp.exp(t - mark)
            z = pltpu.roll(a, HD, 2)
            lo, hi = a[:, :half], a[:, half:]
            ob[c, g * BACK : (g + 1) * BACK] = (
                jnp.where(low_h, z[:, :half], hi).astype(BF16).reshape(flat)
            )
            columns = mark[:, half:]
            columns = jnp.where(lane_h == 0, mark[:, :half], columns)
            columns = jnp.where(lane_h == 2, rounded(lo), columns)
            columns = jnp.where(lane_h == 3, rounded(hi), columns)
            columns = jnp.where(lane_h == 4, lo - rounded(lo), columns)
            columns = jnp.where(lane_h == 5, hi - rounded(hi), columns)
            pick = (iota((2 * 8, LANES), 0) - 8 * g == iota((2 * 8, LANES), 1)) & (
                iota((2 * 8, LANES), 1) < 6
            )
            stats = stats + lax.dot_general(
                jnp.where(pick, 1.0, 0.0).astype(BF16), columns.astype(BF16).reshape(flat), NT,
                preferred_element_type=F32,
            )
        ob[c, BACK:] = stats.astype(BF16)
        copy_o(c).start()

    def copy_o(c):
        return remote(ob.at[c], oin.at[c], s_o, r_o.at[c], target(sp + G, tp))

    missing = jnp.logical_and(col < BACK, group == 0)

    @pl.when(jnp.logical_not(has_prev))
    def _():
        kv[:, own0 - 1] = jnp.zeros((CHUNKS, PIECE, LANES), BF16)

    with scope("h_chunks"):
        @pl.loop(0, CHUNKS)
        def _(c):
            drain(qr.at[c, : G - 1], r_q.at[c])
            drain(kv.at[c, own0 : own0 + halves * (G - 1)], r_kv.at[c])
            kvf[...] = kv[c, own0:].astype(F32)

            @pl.when(has_next)
            def _():
                drain(qb.at[c], r_qb.at[c])
                unpack(qb, c, qbf)
                unpack(qr, c, q2f.at[c], q2)
                run(
                    [*pairs([tile16(c, i, True) for i in each]), [tile4_old(c), tile4_first(c, False)]]
                    + [[tile4(c, n)] for n in range(1, nq // 4)]
                )
                send_old(c)

            @pl.when(jnp.logical_not(has_next))
            def _():
                unpack(qr, c, q2f.at[c], q2)
                run(
                    [*pairs([tile16(c, i, False) for i in each]), [tile4_first(c, True)]]
                    + [[tile4(c, n)] for n in range(1, nq // 4)]
                )

    w_away.start()

    with scope("i_t1"):
        run([[tile1(h)] for h in range(1, nq)])

        @pl.when(has_prev)
        def _():
            drain(kv.at[:, :own0], r_x)
            run([[tile1(0)], *[[tilex(c, i) for i in range(PIECE // 16)] for c in range(CHUNKS)]])

        @pl.when(jnp.logical_not(has_prev))
        def _():
            run([[tile1(0)]])

    eye = jnp.where(iota(flat, 0) == iota(flat, 1), 1.0, 0.0).astype(BF16)
    upper = iota(flat, 0) < HD

    def merge(c, g, extra=False):
        at = slice(g * eight, (g + 1) * eight)
        parts = []
        for sums, tops in ((acc1, top1), (acc4, top4), (acc16, top16), (accx, topx)):
            if sums is accx and not extra:
                continue
            a = sums[c] if sums is accx else sums[c, at]
            t = tops[c] if sums is accx else tops[c, at]
            z = pltpu.roll(a, HD, 2)
            parts.append((
                jnp.where(low_h, z[:, :half], a[:, half:]),
                jnp.where(low_h, a[:, :half], z[:, half:]),
                jnp.where(low_h, t[:, :half], t[:, half:]),
            ))
        t = functools.reduce(jnp.maximum, [part[2] for part in parts])
        scales = [jnp.exp(part[2] - t) for part in parts]
        num = sum(part[0] * scale for part, scale in zip(parts, scales))
        den = sum(part[1] * scale for part, scale in zip(parts, scales))
        return num, den, t

    def finish(c, g, num, den):
        rs[c, g * eight : (g + 1) * eight] = (num / den).astype(BF16).reshape(eight, half, LANES)

    def finish_old(c):
        stats = oin[c, BACK:].astype(F32)

        def spread(j):
            both = jnp.where(
                upper,
                jnp.broadcast_to(stats[j : j + 1], flat),
                jnp.broadcast_to(stats[j + 1 : j + 2], flat),
            )
            return lax.dot_general(eye, both.astype(BF16), NT, preferred_element_type=F32)

        t = pt[c]
        t_old = spread(0)
        t_new = jnp.maximum(t, t_old)
        mine = jnp.exp(t - t_new)
        theirs = jnp.exp(t_old - t_new)
        finish(
            c, 0, pn[c] * mine + oin[c, :BACK].astype(F32) * theirs,
            pd[c] * mine + (spread(2) + spread(4)) * theirs,
        )

    def copy_ret(c, n):
        return remote(
            rs.at[c, n], rr.at[c, head], s_ret, r_ret,
            target(base + n // tp_count, lax.rem(n, tp_count)),
        )

    def give(c, g):
        for o in quad:
            dest = g * hb + lax.rem(mate(o), hb)
            copy_ret(c, dest * tp_count + tp_count - 1 - tp).start()
            if o:
                copy_ret(c, dest * tp_count + tp).start()
            else:
                @pl.when(dest != me)
                def _():
                    copy_ret(c, dest * tp_count + tp).start()

    groups = range(nq // eight)

    with scope("o_finish"):
        @pl.when(has_prev)
        def _():
            for c in range(CHUNKS):
                finish(c, 1, *merge(c, 1, True)[:2])
            for c in range(CHUNKS):
                give(c, 1)
            for c in range(CHUNKS):
                num, den, t = merge(c, 0)
                pn[c] = num.reshape(flat)
                pd[c] = den.reshape(flat)
                pt[c] = t.reshape(flat)

            @pl.loop(0, CHUNKS)
            def _(c):
                drain(oin.at[c], r_o.at[c])
                finish_old(c)
                give(c, 0)

        @pl.when(jnp.logical_not(has_prev))
        def _():
            for c in range(CHUNKS):
                for g in groups:
                    finish(c, g, *merge(c, g)[:2])
            for c in range(CHUNKS):
                for g in groups:
                    give(c, g)

        rr[:, head] = rs[:, seat]

    with scope("q_sendwait"):
        drain(kvs.at[:, : G - 1], s_kv)
        drain(qs.at[:, : G - 1], s_q)

        @pl.when(jnp.logical_and(has_prev, me < hb))
        def _():
            drain(qs, s_qb)

        @pl.when(has_next)
        def _():
            drain(ob, s_o)

        @pl.when(jnp.logical_and(has_next, me >= hb))
        def _():
            drain(kvs, s_x)

        w_local.wait()
        w_away.wait_send()
        pltpu.make_async_remote_copy(
            src_ref=w_ref, dst_ref=wbuf.at[tp_count - 1 - tp],
            send_sem=w_sem.at[1], recv_sem=w_sem.at[2],
            device_id=target(sp, tp_count - 1 - tp), device_id_type=pl.DeviceIdType.MESH,
        ).wait_recv()

    with scope("s_retwait"):
        drain(rr.at[:, : seats - 1], r_ret)

    low_s = iota((half, LANES), 1) < HD
    with scope("t_mix"):
        for m in range(seats // 2):
            x0 = rr[:, 2 * m].astype(F32)
            x1 = rr[:, 2 * m + 1].astype(F32)
            y0 = pltpu.roll(x0, HD, 2)
            y1 = pltpu.roll(x1, HD, 2)
            pair = jnp.concatenate(
                [jnp.where(low_s[None], x0, y1), jnp.where(low_s[None], y0, x1)], axis=1
            ).astype(BF16).reshape(BACK, LANES)
            mx[:, m * LANES : (m + 1) * LANES] = jnp.dot(
                back, pair, preferred_element_type=F32
            ).astype(BF16)

    width = wbuf.shape[1]
    step = 512

    with scope("u_proj"):
        @pl.loop(0, out_ref.shape[1] // step)
        def _(c):
            cols = pl.ds(pl.multiple_of(c * step, step), step)
            total = jnp.dot(mx[:, :width], wbuf[0, :, cols], preferred_element_type=F32)
            total = total + jnp.dot(mx[:, width:], wbuf[1, :, cols], preferred_element_type=F32)
            out_ref[:, cols] = total.astype(BF16)

    with scope("v_end"):
        drain(rs.at[:, : seats - 1], s_ret)


def per_device(sp_count, tp_count, query_rows, key_rows, value_rows, out_weight):
    tok = query_rows.shape[0]
    G = query_rows.shape[1] // HD
    halves = tok // BACK
    ngroups = sp_count // G
    assert tok == 2 * BACK and tp_count == 2 and sp_count % G == 0
    assert G & (G - 1) == 0
    assert G * tok == 16 * BACK
    inverse = np.power(THETA, -np.arange(HD // 2) / (HD // 2))
    inverse = np.tile(inverse, LANES // (HD // 2))[None, :]
    local = np.arange(tok)[:, None] * inverse
    cosb = jnp.asarray(np.cos(local), F32)
    sinb = jnp.asarray(np.sin(local), F32)
    inv = jnp.asarray(np.tile(inverse, (8, 1)), F32)
    seats = G * tp_count
    nq = G * halves
    vmem = pl.BlockSpec(memory_space=pltpu.VMEM)
    dma = pltpu.SemaphoreType.DMA
    return pl.pallas_call(
        functools.partial(kernel, G, ngroups, tp_count),
        out_shape=pltpu.VMEM((tok // tp_count, out_weight.shape[1]), BF16),
        in_specs=[pl.BlockSpec(memory_space=pl.ANY)] * 7,
        out_specs=vmem,
        scratch_shapes=[
            pltpu.VMEM(query_rows.shape, BF16),
            pltpu.VMEM(query_rows.shape, BF16),
            pltpu.VMEM(query_rows.shape, BF16),
            pltpu.VMEM(cosb.shape, F32),
            pltpu.VMEM(sinb.shape, F32),
            pltpu.VMEM(inv.shape, F32),
            pltpu.VMEM((CHUNKS, G, PIECE, LANES), BF16),
            pltpu.VMEM((CHUNKS, G, halves, PIECE, LANES), BF16),
            pltpu.VMEM((CHUNKS, G, PIECE, LANES), BF16),
            pltpu.VMEM((CHUNKS, nq + nq // 2, PIECE, LANES), BF16),
            pltpu.VMEM((nq, PIECE, LANES), F32),
            pltpu.VMEM((CHUNKS, nq, PIECE, LANES), BF16),
            *[pltpu.VMEM((CHUNKS, nq, PIECE, LANES), F32)] * 7,
            *[pltpu.VMEM((CHUNKS, nq // 2, PIECE, LANES), F32)] * 2,
            pltpu.VMEM((CHUNKS, G // 2, PIECE, LANES), BF16),
            *[pltpu.VMEM((nq // 2, PIECE, LANES), F32)] * 3,
            *[pltpu.VMEM((4, PIECE, LANES), F32)] * 2,
            *[pltpu.VMEM((CHUNKS, BACK + 16, LANES), BF16)] * 2,
            *[pltpu.VMEM((CHUNKS, BACK, LANES), F32)] * 3,
            pltpu.VMEM((BACK, 2 * BACK), F32),
            pltpu.VMEM((BACK, 2 * BACK), F32),
            pltpu.VMEM((BACK, 2 * BACK), F32),
            pltpu.VMEM((BACK, BACK), F32),
            pltpu.VMEM((tp_count,) + out_weight.shape, BF16),
            pltpu.VMEM((CHUNKS, seats, PIECE // 2, LANES), BF16),
            pltpu.VMEM((CHUNKS, seats, PIECE // 2, LANES), BF16),
            pltpu.VMEM((BACK, seats * HD), BF16),
            dma, dma, dma, dma, dma, dma,
            dma((CHUNKS,)), dma((CHUNKS,)), dma((CHUNKS,)), dma, dma((CHUNKS,)), dma,
            dma((3,)), dma((6,)),
        ],
        compiler_params=pltpu.CompilerParams(
            collective_id=0, has_side_effects=True, vmem_limit_bytes=63 * 1024 * 1024
        ),
    )(query_rows, key_rows, value_rows, cosb, sinb, inv, out_weight)


def solution(mesh):
    return jax.shard_map(
        functools.partial(per_device, mesh.shape["sp"], mesh.shape["tp"]),
        mesh=mesh,
        in_specs=(P("sp", "tp"), P("sp", "tp"), P("sp", "tp"), P("tp", None)),
        out_specs=P(("sp", "tp"), None),
        check_vma=False,
    )
```

```python
import functools
import math

import jax
import jax.numpy as jnp
import numpy as np
from jax import lax
from jax.experimental import pallas as pl
from jax.experimental.pallas import tpu as pltpu
from jax.sharding import PartitionSpec as P

HD = 64
BACK = 128
THETA = 500000.0
FAR = -1e30
F32 = jnp.float32
BF16 = jnp.bfloat16
LANES = 2 * HD
CHUNKS = 4
PIECE = BACK // CHUNKS
STATS = 16
EARLY = 4
NT = (((1,), (1,)), ((), ()))


def place(p):
    return ((p & 7) << 4) + (((p >> 3) & 3) << 2) + (p >> 5)


def iota(shape, axis):
    return lax.broadcasted_iota(jnp.int32, shape, axis)


def kernel(
    G, ngroups, tp_count,
    q_hbm, k_hbm, v_hbm, cosb_hbm, sinb_hbm, inv_hbm, w_ref, out_ref,
    q_ref, k_ref, v_ref, cosb_ref, sinb_ref, inv_ref, qs, kvs, qr, kv, kvf, q2, q2f,
    acc1, top1, acc4, top4, acc16, top16, accx, topx, qb, qbf, accb, topb, accb4, topb4, ob, oin, pn, pd, pt, b1_ref, b4_ref, b16_ref, bx_ref, wbuf, rs, rr, mx,
    s_kv, s_q, s_qb, s_x, s_y, s_o, s_ret, r_kv, r_q, r_qb, r_x, r_o, r_ret, w_sem, in_sem,
):
    loads = [
        pltpu.make_async_copy(source, dest, in_sem.at[n])
        for n, (source, dest) in enumerate((
            (inv_hbm, inv_ref), (cosb_hbm, cosb_ref), (sinb_hbm, sinb_ref),
            (k_hbm, k_ref), (v_hbm, v_ref), (q_hbm, q_ref),
        ))
    ]
    for load in loads:
        load.start()
    sp = lax.axis_index("sp")
    tp = lax.axis_index("tp")
    group = sp // G
    me = sp - group * G
    base = group * G
    has_prev = group > 0
    has_next = group < ngroups - 1
    seat = me * tp_count + tp
    seats = G * tp_count
    head = tp * G + me
    tok = q_ref.shape[0]
    halves = tok // BACK
    nq = G * halves
    hb = G // 2
    nh = nq // 2
    own0 = nh
    lower = me < hb
    upper = me >= hb

    def target(s, t):
        return {"sp": s, "tp": t}

    barrier = pltpu.get_barrier_semaphore()
    for o in range(1, seats):
        n = lax.rem(seat + o, seats)
        pl.semaphore_signal(
            barrier, inc=1, device_id=target(base + n // tp_count, lax.rem(n, tp_count)),
            device_id_type=pl.DeviceIdType.MESH,
        )

    @pl.when(has_prev)
    def _():
        for o in range(G):
            pl.semaphore_signal(
                barrier, inc=1, device_id=target(base - G + o, tp),
                device_id_type=pl.DeviceIdType.MESH,
            )

    @pl.when(has_next)
    def _():
        for o in range(G):
            pl.semaphore_signal(
                barrier, inc=1, device_id=target(base + G + o, tp),
                device_id_type=pl.DeviceIdType.MESH,
            )

    w_local = pltpu.make_async_copy(w_ref, wbuf.at[tp], w_sem.at[0])
    w_local.start()

    def stride4(n):
        w = n & 31
        return ((n >> 5) << 5) + ((w & 7) << 2) + (w >> 3)

    def masked(distance):
        return jnp.where((distance >= 0) & (distance <= BACK), 0.0, FAR)

    row = iota((BACK, 2 * BACK), 0)
    col = iota((BACK, 2 * BACK), 1)
    b1_ref[...] = masked(place(row) + BACK - place(col & (BACK - 1)) - ((col >> 7) << 7))
    b4_ref[...] = masked(stride4(row) + BACK - stride4(col))
    b16_ref[...] = masked(row + BACK - col)

    def stride16(n):
        return ((n >> 4) << 3) + (n & 7)

    xrow = iota((BACK, BACK), 0)
    xcol = iota((BACK, BACK), 1)
    same = ((xrow ^ xcol) & 8) == 0
    bx_ref[...] = jnp.where(same, masked(stride16(xrow) + BACK - stride16(xcol)), FAR)

    scope = jax.named_scope
    with scope("a_loads"):
        for load in loads:
            load.wait()

    lane = iota((BACK, LANES), 1)
    low = lane < HD
    lane_t = iota((tok, LANES), 1)
    first = (lane_t & (HD - 1)) < HD // 2
    angle = inv_ref[...] * (sp * tok).astype(F32)
    ca = jnp.cos(angle)[:1]
    sa = jnp.sin(angle)[:1]
    cos = ca * cosb_ref[...] - sa * sinb_ref[...]
    sin = sa * cosb_ref[...] + ca * sinb_ref[...]
    sin = jnp.where(first, -sin, sin)
    swizzle = jnp.where(place(iota((BACK, BACK), 0)) == iota((BACK, BACK), 1), 1.0, 0.0).astype(BF16)
    back = jnp.where(place(iota((BACK, BACK), 1)) == iota((BACK, BACK), 0), 1.0, 0.0).astype(BF16)

    def turn(ref, cols):
        x = ref[:, cols].astype(F32)
        other = jnp.where(first, pltpu.roll(x, LANES - HD // 2, 1), pltpu.roll(x, HD // 2, 1))
        return (x * cos + other * sin).astype(BF16)

    def sw(x):
        return jnp.dot(swizzle, x, preferred_element_type=F32)

    def cut(x):
        return x.astype(BF16).reshape(CHUNKS, PIECE, LANES)

    with scope("c_turn"):
        for m in range(G // 2):
            cols = slice(m * LANES, (m + 1) * LANES)
            tq = turn(q_ref, cols)
            tk = turn(k_ref, cols)
            tv = v_ref[:, cols]
            q_a = sw(tq[:BACK]) * (1.0 / math.sqrt(HD))
            q_b = sw(tq[BACK:]) * (1.0 / math.sqrt(HD))
            qs[:, 2 * m] = cut(jnp.where(low, q_a, pltpu.roll(q_b, HD, 1)))
            qs[:, 2 * m + 1] = cut(jnp.where(low, pltpu.roll(q_a, HD, 1), q_b))
            for e in range(halves):
                ks = sw(tk[e * BACK : (e + 1) * BACK])
                vs = sw(tv[e * BACK : (e + 1) * BACK])
                kvs[:, 2 * m, e] = cut(jnp.where(low, ks, pltpu.roll(vs, HD, 1)))
                kvs[:, 2 * m + 1, e] = cut(jnp.where(low, pltpu.roll(ks, HD, 1), vs))

    with scope("d_barrier"):
        pl.semaphore_wait(
            barrier, seats - 1 + jnp.where(has_prev, G, 0) + jnp.where(has_next, G, 0)
        )

    def remote(source, dest, send, recv, device):
        return pltpu.make_async_remote_copy(
            src_ref=source, dst_ref=dest, send_sem=send, recv_sem=recv,
            device_id=device, device_id_type=pl.DeviceIdType.MESH,
        )

    def drain(ref, sem):
        pltpu.make_async_copy(ref, ref, sem).wait()

    def copy_kv(c, dest):
        return remote(
            kvs.at[c, dest], kv.at[c, pl.ds(own0 + halves * me, halves)],
            s_kv, r_kv.at[c], target(base + dest, tp),
        )

    def copy_q(c, dest):
        return remote(qs.at[c, dest], qr.at[c, me], s_q, r_q.at[c], target(base + dest, tp))

    def copy_qb(c, dest):
        return remote(
            qs.at[c, dest], qb.at[c, me], s_qb, r_qb.at[c], target(base - G + dest, tp)
        )

    def copy_y(c, dest):
        return remote(
            kvs.at[c, dest, halves - 1], kv.at[c, own0 - 1], s_y, r_x, target(base + G + dest, tp)
        )

    def copy_x(c, dest):
        return remote(
            kvs.at[c, dest], kv.at[c, pl.ds(halves * (me - hb), halves)],
            s_x, r_x, target(base + G + dest, tp),
        )

    w_away = pltpu.make_async_remote_copy(
        src_ref=w_ref, dst_ref=wbuf.at[tp], send_sem=w_sem.at[1], recv_sem=w_sem.at[2],
        device_id=target(sp, tp_count - 1 - tp), device_id_type=pl.DeviceIdType.MESH,
    )

    bits = [1 << n for n in range(G.bit_length() - 1)]
    far = sorted(range(1, G), key=lambda o: -o.bit_count())

    quad = [o for o in far if o < hb] + [0]

    def mate(o):
        return sum((((me // b + o // b) % 2) * b for b in bits), 0)

    def send_back(c):
        @pl.when(jnp.logical_and(has_prev, lower))
        def _():
            for o in [*far, 0]:
                copy_qb(c, mate(o)).start()

        @pl.when(jnp.logical_and(has_prev, upper))
        def _():
            for o in quad:
                copy_qb(c, hb + lax.rem(mate(o), hb)).start()

    with scope("e_issue"):
        @pl.when(jnp.logical_and(has_next, upper))
        def _():
            for c in range(CHUNKS):
                for o in quad:
                    copy_x(c, lax.rem(mate(o), hb)).start()

        @pl.when(jnp.logical_and(has_next, me == G - 1))
        def _():
            for c in range(CHUNKS):
                for o in quad:
                    copy_y(c, hb + lax.rem(mate(o), hb)).start()

        for c in range(CHUNKS):
            if c < EARLY:
                send_back(c)
            for o in far:
                copy_q(c, mate(o)).start()
                copy_kv(c, mate(o)).start()

    for c in range(CHUNKS):
        kv[c, pl.ds(own0 + halves * me, halves)] = kvs[c, me]
        qr[c, me] = qs[c, me]

    low_p = low[:PIECE]

    def unpack(ref, c, sources, wide, narrow=None):
        for s in range(sources):
            x = ref[c, s].astype(F32)
            a = jnp.where(low_p, x, 0.0)
            b = jnp.where(low_p, pltpu.roll(x, HD, 1), 0.0)
            wide[2 * s] = a
            wide[2 * s + 1] = b
            if narrow is not None:
                narrow[c, 2 * s] = a.astype(BF16)
                narrow[c, 2 * s + 1] = b.astype(BF16)

    def run(tiles):
        done = []
        for tile in tiles:
            q = jnp.concatenate([part[0] for part in tile], axis=0)
            keys = jnp.concatenate([part[1] for part in tile], axis=0)
            s = lax.dot_general(q, keys, NT, preferred_element_type=F32)
            rows, cols, ps, ts = 0, 0, [], []
            for part in tile:
                n, k = part[0].shape[0], part[1].shape[0]
                mine = s[rows : rows + n, cols : cols + k] + part[2]
                t = jnp.max(mine, axis=1, keepdims=True)
                p = [
                    jnp.exp(mine[:, a : a + LANES] - t).astype(BF16) for a in range(0, k, LANES)
                ]
                none = jnp.zeros_like(p[0])
                before, after = cols // LANES, (keys.shape[0] - cols - k) // LANES
                ps.append(jnp.concatenate([none] * before + p + [none] * after, axis=1))
                ts.append(t)
                rows, cols = rows + n, cols + k
            ones = jnp.where(iota(keys.shape, 1) < HD, jnp.ones_like(keys), keys)
            o = jnp.dot(jnp.concatenate(ps, axis=0), ones, preferred_element_type=F32)
            rows = 0
            for part, t in zip(tile, ts):
                end = rows + part[0].shape[0]
                done.append((part[3], o[rows:end], jnp.broadcast_to(t, (end - rows, LANES))))
                rows = end
        for places, o, t in done:
            first_row = 0
            for sums, tops, at in places:
                shape = sums[at].shape
                rows = slice(first_row, first_row + math.prod(shape[:-1]))
                sums[at] = o[rows].reshape(shape)
                tops[at] = t[rows].reshape(shape)
                first_row = rows.stop

    def pairs(tiles):
        return [tiles[n : n + 2] for n in range(0, len(tiles), 2)]

    every = slice(None)

    def block(h):
        return kv[:, own0 + h].reshape(BACK, LANES)

    def tile1(h):
        return (
            q2[:, h].reshape(BACK, LANES), jnp.concatenate([block(h - 1), block(h)], axis=0),
            jnp.where(missing, FAR, b1_ref[...]) if h == 0 else b1_ref[...],
            ((acc1, top1, (every, h)),),
        )

    def tile4(c, n):
        blocks = slice(4 * n, 4 * n + 4)
        return (
            q2[c, blocks].reshape(BACK, LANES),
            kv[c, own0 + 4 * n - 4 : own0 + 4 * n + 4].reshape(2 * BACK, LANES),
            b4_ref[...], ((acc4, top4, (c, blocks)),),
        )

    def tile4_first(c, alone):
        keys = kv[c, own0 : own0 + 4].reshape(BACK, LANES)
        b = b4_ref[:, BACK:]
        if alone:
            keys = jnp.concatenate([keys, keys], axis=0)
            b = jnp.concatenate([jnp.full_like(b, FAR), b], axis=1)
        return (q2[c, :4].reshape(BACK, LANES), keys, b, ((acc4, top4, (c, slice(0, 4))),))

    def tile4_old(c):
        return (
            qbf[:4].reshape(BACK, LANES).astype(BF16),
            kv[c, own0 + nq - 4 : own0 + nq].reshape(BACK, LANES),
            b4_ref[:, :BACK], ((accb4, topb4, (every,)),),
        )

    def tile16(c, i, olds):
        rows = slice(8 * i, 8 * i + 8)
        q = q2f[c, :, rows].reshape(BACK, LANES).astype(BF16)
        b = b16_ref[:, BACK:]
        places = ((acc16, top16, (c, every, rows)),)
        if olds:
            old = qbf[:olds, rows].reshape(-1, LANES).astype(BF16)
            q = jnp.concatenate([q, old], axis=0)
            b = jnp.concatenate([b, b16_ref[: old.shape[0], :BACK]], axis=0)
            places = (*places, (accb, topb, (slice(0, olds), rows)))
        return (q, kvf[:, rows].reshape(BACK, LANES).astype(BF16), b, places)

    def tilex(c, i):
        rows = slice(16 * i, 16 * i + 16)
        return (
            q2[c, nh:, rows].reshape(BACK, LANES), kv[c, :nh, rows].reshape(BACK, LANES),
            bx_ref[...], ((accx, topx, (c, every, rows)),),
        )

    each = range(PIECE // 8)
    half = PIECE // 2
    eight = BACK // half
    lane_h = iota((eight, half, LANES), 2)
    low_h = lane_h < HD
    flat = (BACK, LANES)

    def rounded(x):
        return x.astype(BF16).astype(F32)

    def send_old(c, olds):
        t4, t16 = topb4[...], topb[:4]
        t = jnp.maximum(t4, t16)
        accb[:4] = accb[:4] * jnp.exp(t16 - t) + accb4[...] * jnp.exp(t4 - t)
        topb[:4] = t
        stats = jnp.zeros((STATS, LANES), F32)
        for g in range(olds // eight):
            at = slice(g * eight, (g + 1) * eight)
            t = topb[at]
            mark = rounded(t)
            a = accb[at] * jnp.exp(t - mark)
            z = pltpu.roll(a, HD, 2)
            lo, hi = a[:, :half], a[:, half:]
            ob[c, STATS + g * BACK : STATS + (g + 1) * BACK] = (
                jnp.where(low_h, z[:, :half], hi).astype(BF16).reshape(flat)
            )
            columns = mark[:, half:]
            columns = jnp.where(lane_h == 0, mark[:, :half], columns)
            columns = jnp.where(lane_h == 2, rounded(lo), columns)
            columns = jnp.where(lane_h == 3, rounded(hi), columns)
            columns = jnp.where(lane_h == 4, lo - rounded(lo), columns)
            columns = jnp.where(lane_h == 5, hi - rounded(hi), columns)
            pick = (iota((STATS, LANES), 0) - 8 * g == iota((STATS, LANES), 1)) & (
                iota((STATS, LANES), 1) < 6
            )
            stats = stats + lax.dot_general(
                jnp.where(pick, 1.0, 0.0).astype(BF16), columns.astype(BF16).reshape(flat), NT,
                preferred_element_type=F32,
            )
        ob[c, :STATS] = stats.astype(BF16)
        copy_o(c, olds).start()

    def old_rows(olds):
        return slice(0, STATS + olds * half)

    def copy_o(c, olds):
        at = old_rows(olds)
        return remote(ob.at[c, at], oin.at[c, at], s_o, r_o.at[c], target(sp + G, tp))

    def blend(c):
        t4, t16 = top4[c], top16[c]
        t = jnp.maximum(t4, t16)
        acc16[c] = acc4[c] * jnp.exp(t4 - t) + acc16[c] * jnp.exp(t16 - t)
        top16[c] = t

    missing = jnp.logical_and(col < BACK, group == 0)

    @pl.when(jnp.logical_not(has_prev))
    def _():
        kv[:, own0 - 1] = jnp.zeros((CHUNKS, PIECE, LANES), BF16)

    with scope("h_chunks"):
        @pl.loop(0, CHUNKS)
        def _(c):
            drain(qr.at[c, : G - 1], r_q.at[c])
            drain(kv.at[c, own0 : own0 + halves * (G - 1)], r_kv.at[c])
            kvf[...] = kv[c, own0:].astype(F32)


            def serve(olds):
                if olds:
                    drain(qb.at[c, : olds // halves], r_qb.at[c])
                    unpack(qb, c, olds // halves, qbf)
                unpack(qr, c, G, q2f.at[c], q2)
                four = [tile4_old(c), tile4_first(c, False)] if olds else [tile4_first(c, True)]
                run(
                    [*pairs([tile16(c, i, olds) for i in each]), four]
                    + [[tile4(c, n)] for n in range(1, nq // 4)]
                )
                if olds:
                    send_old(c, olds)
                blend(c)

            @pl.when(jnp.logical_and(has_next, lower))
            def _():
                serve(nh)

            @pl.when(jnp.logical_and(has_next, upper))
            def _():
                serve(nq)

            @pl.when(jnp.logical_not(has_next))
            def _():
                serve(0)

    w_away.start()

    with scope("i_t1"):
        run([[tile1(h)] for h in range(1, nq)])

        @pl.when(jnp.logical_and(has_prev, lower))
        def _():
            drain(kv.at[:, :own0], r_x)
            run([[tile1(0)], *[[tilex(c, i) for i in range(PIECE // 16)] for c in range(CHUNKS)]])

        @pl.when(jnp.logical_and(has_prev, upper))
        def _():
            drain(kv.at[:, own0 - 1], r_x)
            run([[tile1(0)]])

        @pl.when(jnp.logical_not(has_prev))
        def _():
            run([[tile1(0)]])

    eye = jnp.where(iota(flat, 0) == iota(flat, 1), 1.0, 0.0).astype(BF16)
    top_rows = iota(flat, 0) < HD

    def merge(c, g, extra=False):
        at = slice(g * eight, (g + 1) * eight)
        parts = [(acc1[c, at], top1[c, at]), (acc16[c, at], top16[c, at])]
        if extra:
            parts.append((accx[c], topx[c]))
        t = functools.reduce(jnp.maximum, [part[1] for part in parts])
        a = sum(part[0] * jnp.exp(part[1] - t) for part in parts)
        z = pltpu.roll(a, HD, 2)
        return (
            jnp.where(low_h, z[:, :half], a[:, half:]),
            jnp.where(low_h, a[:, :half], z[:, half:]),
            jnp.where(low_h, t[:, :half], t[:, half:]),
        )

    def finish(c, g, num, den):
        rs[c, g * eight : (g + 1) * eight] = (num / den).astype(BF16).reshape(eight, half, LANES)

    def finish_old(c, g):
        stats = oin[c, :STATS].astype(F32)

        def spread(j):
            at = 8 * g + j
            both = jnp.where(
                top_rows,
                jnp.broadcast_to(stats[at : at + 1], flat),
                jnp.broadcast_to(stats[at + 1 : at + 2], flat),
            )
            return lax.dot_general(eye, both.astype(BF16), NT, preferred_element_type=F32)

        t = pt[c, g]
        t_old = spread(0)
        t_new = jnp.maximum(t, t_old)
        mine = jnp.exp(t - t_new)
        theirs = jnp.exp(t_old - t_new)
        old = oin[c, STATS + g * BACK : STATS + (g + 1) * BACK].astype(F32)
        finish(
            c, g, pn[c, g] * mine + old * theirs,
            pd[c, g] * mine + (spread(2) + spread(4)) * theirs,
        )

    def copy_ret(c, n):
        return remote(
            rs.at[c, n], rr.at[c, head], s_ret, r_ret,
            target(base + n // tp_count, lax.rem(n, tp_count)),
        )

    def give(c, g):
        for o in quad:
            dest = g * hb + lax.rem(mate(o), hb)
            copy_ret(c, dest * tp_count + tp_count - 1 - tp).start()
            if o:
                copy_ret(c, dest * tp_count + tp).start()
            else:
                @pl.when(dest != me)
                def _():
                    copy_ret(c, dest * tp_count + tp).start()

    groups = range(nq // eight)

    def close(olds, late):
        for c in range(CHUNKS):
            for g in late:
                num, den, t = merge(c, g)
                pn[c, g] = num.reshape(flat)
                pd[c, g] = den.reshape(flat)
                pt[c, g] = t.reshape(flat)

        @pl.loop(0, CHUNKS // 2)
        def _(i):
            for c in (2 * i, 2 * i + 1):
                drain(oin.at[c, old_rows(olds)], r_o.at[c])
            for c in (2 * i, 2 * i + 1):
                for g in late:
                    finish_old(c, g)
            for c in (2 * i, 2 * i + 1):
                for g in late:
                    give(c, g)

    with scope("o_finish"):
        @pl.when(jnp.logical_and(has_prev, lower))
        def _():
            for c in range(CHUNKS):
                finish(c, 1, *merge(c, 1, True)[:2])
            for c in range(CHUNKS):
                give(c, 1)
            close(nh, (0,))

        @pl.when(jnp.logical_and(has_prev, upper))
        def _():
            close(nq, (0, 1))

        @pl.when(jnp.logical_not(has_prev))
        def _():
            for c in range(CHUNKS):
                for g in groups:
                    finish(c, g, *merge(c, g)[:2])
            for c in range(CHUNKS):
                for g in groups:
                    give(c, g)

        rr[:, head] = rs[:, seat]

    with scope("q_sendwait"):
        drain(kvs.at[:, : G - 1], s_kv)
        drain(qs.at[:, : G - 1], s_q)

        @pl.when(jnp.logical_and(has_prev, lower))
        def _():
            drain(qs, s_qb)

        @pl.when(jnp.logical_and(has_prev, upper))
        def _():
            drain(qs.at[:, :hb], s_qb)

        @pl.when(jnp.logical_and(has_next, lower))
        def _():
            drain(ob.at[:, old_rows(nh)], s_o)

        @pl.when(jnp.logical_and(has_next, upper))
        def _():
            drain(ob, s_o)
            drain(kvs.at[:, :hb], s_x)

        @pl.when(jnp.logical_and(has_next, me == G - 1))
        def _():
            drain(kvs.at[:, :hb, halves - 1], s_y)

        w_local.wait()
        w_away.wait_send()
        pltpu.make_async_remote_copy(
            src_ref=w_ref, dst_ref=wbuf.at[tp_count - 1 - tp],
            send_sem=w_sem.at[1], recv_sem=w_sem.at[2],
            device_id=target(sp, tp_count - 1 - tp), device_id_type=pl.DeviceIdType.MESH,
        ).wait_recv()

    with scope("s_retwait"):
        drain(rr.at[:, : seats - 1], r_ret)

    low_s = iota((half, LANES), 1) < HD
    with scope("t_mix"):
        for m in range(seats // 2):
            x0 = rr[:, 2 * m].astype(F32)
            x1 = rr[:, 2 * m + 1].astype(F32)
            y0 = pltpu.roll(x0, HD, 2)
            y1 = pltpu.roll(x1, HD, 2)
            pair = jnp.concatenate(
                [jnp.where(low_s[None], x0, y1), jnp.where(low_s[None], y0, x1)], axis=1
            ).astype(BF16).reshape(BACK, LANES)
            mx[:, m * LANES : (m + 1) * LANES] = jnp.dot(
                back, pair, preferred_element_type=F32
            ).astype(BF16)

    width = wbuf.shape[1]
    step = 2048

    with scope("u_proj"):
        @pl.loop(0, out_ref.shape[1] // step)
        def _(c):
            cols = pl.ds(pl.multiple_of(c * step, step), step)
            total = jnp.dot(mx[:, :width], wbuf[0, :, cols], preferred_element_type=F32)
            total = total + jnp.dot(mx[:, width:], wbuf[1, :, cols], preferred_element_type=F32)
            out_ref[:, cols] = total.astype(BF16)

    with scope("v_end"):
        drain(rs.at[:, : seats - 1], s_ret)


def per_device(sp_count, tp_count, query_rows, key_rows, value_rows, out_weight):
    tok = query_rows.shape[0]
    G = query_rows.shape[1] // HD
    halves = tok // BACK
    ngroups = sp_count // G
    assert tok == 2 * BACK and tp_count == 2 and sp_count % G == 0
    assert G & (G - 1) == 0
    assert G * tok == 16 * BACK
    inverse = np.power(THETA, -np.arange(HD // 2) / (HD // 2))
    inverse = np.tile(inverse, LANES // (HD // 2))[None, :]
    local = np.arange(tok)[:, None] * inverse
    cosb = jnp.asarray(np.cos(local), F32)
    sinb = jnp.asarray(np.sin(local), F32)
    inv = jnp.asarray(np.tile(inverse, (8, 1)), F32)
    seats = G * tp_count
    nq = G * halves
    vmem = pl.BlockSpec(memory_space=pltpu.VMEM)
    dma = pltpu.SemaphoreType.DMA
    return pl.pallas_call(
        functools.partial(kernel, G, ngroups, tp_count),
        out_shape=pltpu.VMEM((tok // tp_count, out_weight.shape[1]), BF16),
        in_specs=[pl.BlockSpec(memory_space=pl.ANY)] * 7,
        out_specs=vmem,
        scratch_shapes=[
            pltpu.VMEM(query_rows.shape, BF16),
            pltpu.VMEM(query_rows.shape, BF16),
            pltpu.VMEM(query_rows.shape, BF16),
            pltpu.VMEM(cosb.shape, F32),
            pltpu.VMEM(sinb.shape, F32),
            pltpu.VMEM(inv.shape, F32),
            pltpu.VMEM((CHUNKS, G, PIECE, LANES), BF16),
            pltpu.VMEM((CHUNKS, G, halves, PIECE, LANES), BF16),
            pltpu.VMEM((CHUNKS, G, PIECE, LANES), BF16),
            pltpu.VMEM((CHUNKS, nq + nq // 2, PIECE, LANES), BF16),
            pltpu.VMEM((nq, PIECE, LANES), F32),
            pltpu.VMEM((CHUNKS, nq, PIECE, LANES), BF16),
            *[pltpu.VMEM((CHUNKS, nq, PIECE, LANES), F32)] * 7,
            *[pltpu.VMEM((CHUNKS, nq // 2, PIECE, LANES), F32)] * 2,
            pltpu.VMEM((CHUNKS, G, PIECE, LANES), BF16),
            *[pltpu.VMEM((nq, PIECE, LANES), F32)] * 3,
            *[pltpu.VMEM((4, PIECE, LANES), F32)] * 2,
            *[pltpu.VMEM((CHUNKS, STATS + nq * PIECE // 2, LANES), BF16)] * 2,
            *[pltpu.VMEM((CHUNKS, nq * PIECE // (2 * BACK), BACK, LANES), F32)] * 3,
            pltpu.VMEM((BACK, 2 * BACK), F32),
            pltpu.VMEM((BACK, 2 * BACK), F32),
            pltpu.VMEM((BACK, 2 * BACK), F32),
            pltpu.VMEM((BACK, BACK), F32),
            pltpu.VMEM((tp_count,) + out_weight.shape, BF16),
            pltpu.VMEM((CHUNKS, seats, PIECE // 2, LANES), BF16),
            pltpu.VMEM((CHUNKS, seats, PIECE // 2, LANES), BF16),
            pltpu.VMEM((BACK, seats * HD), BF16),
            dma, dma, dma, dma, dma, dma, dma,
            dma((CHUNKS,)), dma((CHUNKS,)), dma((CHUNKS,)), dma, dma((CHUNKS,)), dma,
            dma((3,)), dma((6,)),
        ],
        compiler_params=pltpu.CompilerParams(
            collective_id=0, has_side_effects=True, vmem_limit_bytes=63 * 1024 * 1024
        ),
    )(query_rows, key_rows, value_rows, cosb, sinb, inv, out_weight)


def solution(mesh):
    return jax.shard_map(
        functools.partial(per_device, mesh.shape["sp"], mesh.shape["tp"]),
        mesh=mesh,
        in_specs=(P("sp", "tp"), P("sp", "tp"), P("sp", "tp"), P("tp", None)),
        out_specs=P(("sp", "tp"), None),
        check_vma=False,
    )
```

```python
import functools
import math

import jax
import jax.numpy as jnp
import numpy as np
from jax import lax
from jax.experimental import pallas as pl
from jax.experimental.pallas import tpu as pltpu
from jax.sharding import PartitionSpec as P

HD = 64
BACK = 128
THETA = 500000.0
FAR = -1e30
F32 = jnp.float32
BF16 = jnp.bfloat16
LANES = 2 * HD
CHUNKS = 4
PIECE = BACK // CHUNKS
STATS = 16
NT = (((1,), (1,)), ((), ()))


def place(p):
    return ((p & 7) << 4) + (((p >> 3) & 3) << 2) + (p >> 5)


def iota(shape, axis):
    return lax.broadcasted_iota(jnp.int32, shape, axis)


def kernel(
    G, ngroups, tp_count,
    q_hbm, k_hbm, v_hbm, cosb_hbm, sinb_hbm, inv_hbm, w_ref, out_ref,
    q_ref, k_ref, v_ref, cosb_ref, sinb_ref, inv_ref, qs, kvs, qr, kv, kvf, q2, q2f,
    acc1, top1, acc4, top4, acc16, top16, accx, topx, qb, qbf, accb, topb, accb4, topb4, ob, oin, pn, pd, pt, b1_ref, b4_ref, b16_ref, bx_ref, wbuf, rs, rr, mx,
    s_kv, s_q, s_qb, s_x, s_y, s_o, s_ret, r_kv, r_q, r_qb, r_x, r_o, r_ret, w_sem, in_sem,
):
    loads = [
        pltpu.make_async_copy(source, dest, in_sem.at[n])
        for n, (source, dest) in enumerate((
            (inv_hbm, inv_ref), (cosb_hbm, cosb_ref), (sinb_hbm, sinb_ref),
            (k_hbm, k_ref), (v_hbm, v_ref), (q_hbm, q_ref),
        ))
    ]
    for load in loads:
        load.start()
    sp = lax.axis_index("sp")
    tp = lax.axis_index("tp")
    group = sp // G
    me = sp - group * G
    base = group * G
    has_prev = group > 0
    has_next = group < ngroups - 1
    seat = me * tp_count + tp
    seats = G * tp_count
    head = tp * G + me
    tok = q_ref.shape[0]
    halves = tok // BACK
    nq = G * halves
    hb = G // 2
    nh = nq // 2
    own0 = nh
    lower = me < hb
    upper = me >= hb

    def target(s, t):
        return {"sp": s, "tp": t}

    barrier = pltpu.get_barrier_semaphore()
    for o in range(1, seats):
        n = lax.rem(seat + o, seats)
        pl.semaphore_signal(
            barrier, inc=1, device_id=target(base + n // tp_count, lax.rem(n, tp_count)),
            device_id_type=pl.DeviceIdType.MESH,
        )

    @pl.when(has_prev)
    def _():
        for o in range(G):
            pl.semaphore_signal(
                barrier, inc=1, device_id=target(base - G + o, tp),
                device_id_type=pl.DeviceIdType.MESH,
            )

    @pl.when(has_next)
    def _():
        for o in range(G):
            pl.semaphore_signal(
                barrier, inc=1, device_id=target(base + G + o, tp),
                device_id_type=pl.DeviceIdType.MESH,
            )

    w_local = pltpu.make_async_copy(w_ref, wbuf.at[tp], w_sem.at[0])
    w_local.start()

    def stride4(n):
        w = n & 31
        return ((n >> 5) << 5) + ((w & 7) << 2) + (w >> 3)

    def masked(distance):
        return jnp.where((distance >= 0) & (distance <= BACK), 0.0, FAR)

    row = iota((BACK, 2 * BACK), 0)
    col = iota((BACK, 2 * BACK), 1)
    b1_ref[...] = masked(place(row) + BACK - place(col & (BACK - 1)) - ((col >> 7) << 7))
    b4_ref[...] = masked(stride4(row) + BACK - stride4(col))
    b16_ref[...] = masked(row + BACK - col)

    def stride16(n):
        return ((n >> 4) << 3) + (n & 7)

    xrow = iota((BACK, BACK), 0)
    xcol = iota((BACK, BACK), 1)
    same = ((xrow ^ xcol) & 8) == 0
    bx_ref[...] = jnp.where(same, masked(stride16(xrow) + BACK - stride16(xcol)), FAR)

    scope = jax.named_scope
    with scope("a_loads"):
        for load in loads:
            load.wait()

    lane = iota((BACK, LANES), 1)
    low = lane < HD
    lane_t = iota((tok, LANES), 1)
    first = (lane_t & (HD - 1)) < HD // 2
    angle = inv_ref[...] * (sp * tok).astype(F32)
    ca = jnp.cos(angle)[:1]
    sa = jnp.sin(angle)[:1]
    cos = ca * cosb_ref[...] - sa * sinb_ref[...]
    sin = sa * cosb_ref[...] + ca * sinb_ref[...]
    sin = jnp.where(first, -sin, sin)
    swizzle = jnp.where(place(iota((BACK, BACK), 0)) == iota((BACK, BACK), 1), 1.0, 0.0).astype(BF16)
    back = jnp.where(place(iota((BACK, BACK), 1)) == iota((BACK, BACK), 0), 1.0, 0.0).astype(BF16)

    def turn(ref, cols):
        x = ref[:, cols].astype(F32)
        other = jnp.where(first, pltpu.roll(x, LANES - HD // 2, 1), pltpu.roll(x, HD // 2, 1))
        return (x * cos + other * sin).astype(BF16)

    def sw(x):
        return jnp.dot(swizzle, x, preferred_element_type=F32)

    def cut(x):
        return x.astype(BF16).reshape(CHUNKS, PIECE, LANES)

    with scope("c_turn"):
        for m in range(G // 2):
            cols = slice(m * LANES, (m + 1) * LANES)
            tq = turn(q_ref, cols)
            tk = turn(k_ref, cols)
            tv = v_ref[:, cols]
            q_a = sw(tq[:BACK]) * (1.0 / math.sqrt(HD))
            q_b = sw(tq[BACK:]) * (1.0 / math.sqrt(HD))
            qs[:, 2 * m] = cut(jnp.where(low, q_a, pltpu.roll(q_b, HD, 1)))
            qs[:, 2 * m + 1] = cut(jnp.where(low, pltpu.roll(q_a, HD, 1), q_b))
            for e in range(halves):
                ks = sw(tk[e * BACK : (e + 1) * BACK])
                vs = sw(tv[e * BACK : (e + 1) * BACK])
                kvs[:, 2 * m, e] = cut(jnp.where(low, ks, pltpu.roll(vs, HD, 1)))
                kvs[:, 2 * m + 1, e] = cut(jnp.where(low, pltpu.roll(ks, HD, 1), vs))

    with scope("d_barrier"):
        pl.semaphore_wait(
            barrier, seats - 1 + jnp.where(has_prev, G, 0) + jnp.where(has_next, G, 0)
        )

    def remote(source, dest, send, recv, device):
        return pltpu.make_async_remote_copy(
            src_ref=source, dst_ref=dest, send_sem=send, recv_sem=recv,
            device_id=device, device_id_type=pl.DeviceIdType.MESH,
        )

    def drain(ref, sem):
        pltpu.make_async_copy(ref, ref, sem).wait()

    def copy_kv(c, dest):
        return remote(
            kvs.at[c, dest], kv.at[c, pl.ds(own0 + halves * me, halves)],
            s_kv, r_kv.at[c], target(base + dest, tp),
        )

    def copy_q(c, dest):
        return remote(qs.at[c, dest], qr.at[c, me], s_q, r_q.at[c], target(base + dest, tp))

    def copy_qb(c, dest):
        return remote(
            qs.at[c, dest], qb.at[c, me], s_qb, r_qb.at[c], target(base - G + dest, tp)
        )

    def copy_y(c, dest):
        return remote(
            kvs.at[c, dest, halves - 1], kv.at[c, own0 - 1], s_y, r_x, target(base + G + dest, tp)
        )

    def copy_x(c, dest):
        return remote(
            kvs.at[c, dest], kv.at[c, pl.ds(halves * (me - hb), halves)],
            s_x, r_x, target(base + G + dest, tp),
        )

    w_away = pltpu.make_async_remote_copy(
        src_ref=w_ref, dst_ref=wbuf.at[tp], send_sem=w_sem.at[1], recv_sem=w_sem.at[2],
        device_id=target(sp, tp_count - 1 - tp), device_id_type=pl.DeviceIdType.MESH,
    )

    bits = [1 << n for n in range(G.bit_length() - 1)]
    far = sorted(range(1, G), key=lambda o: -o.bit_count())

    quad = [o for o in far if o < hb] + [0]

    def mate(o):
        return sum((((me // b + o // b) % 2) * b for b in bits), 0)

    def send_back(c):
        @pl.when(jnp.logical_and(has_prev, lower))
        def _():
            for o in [*far, 0]:
                copy_qb(c, mate(o)).start()

        @pl.when(jnp.logical_and(has_prev, upper))
        def _():
            for o in quad:
                copy_qb(c, hb + lax.rem(mate(o), hb)).start()

    with scope("e_issue"):
        @pl.when(jnp.logical_and(has_next, upper))
        def _():
            for c in range(CHUNKS):
                for o in quad:
                    copy_x(c, lax.rem(mate(o), hb)).start()

        @pl.when(jnp.logical_and(has_next, me == G - 1))
        def _():
            for c in range(CHUNKS):
                for o in quad:
                    copy_y(c, hb + lax.rem(mate(o), hb)).start()

        for c in range(CHUNKS):
            send_back(c)
            for o in far:
                copy_q(c, mate(o)).start()
                copy_kv(c, mate(o)).start()

    for c in range(CHUNKS):
        kv[c, pl.ds(own0 + halves * me, halves)] = kvs[c, me]
        qr[c, me] = qs[c, me]

    low_p = low[:PIECE]

    def unpack(ref, c, sources, wide, narrow=None):
        for s in range(sources):
            x = ref[c, s].astype(F32)
            a = jnp.where(low_p, x, 0.0)
            b = jnp.where(low_p, pltpu.roll(x, HD, 1), 0.0)
            wide[2 * s] = a
            wide[2 * s + 1] = b
            if narrow is not None:
                narrow[c, 2 * s] = a.astype(BF16)
                narrow[c, 2 * s + 1] = b.astype(BF16)

    def run(tiles):
        done = []
        for tile in tiles:
            q = jnp.concatenate([part[0] for part in tile], axis=0)
            keys = jnp.concatenate([part[1] for part in tile], axis=0)
            s = lax.dot_general(q, keys, NT, preferred_element_type=F32)
            rows, cols, ps, ts = 0, 0, [], []
            for part in tile:
                n, k = part[0].shape[0], part[1].shape[0]
                mine = s[rows : rows + n, cols : cols + k] + part[2]
                t = jnp.max(mine, axis=1, keepdims=True)
                p = [
                    jnp.exp(mine[:, a : a + LANES] - t).astype(BF16) for a in range(0, k, LANES)
                ]
                none = jnp.zeros_like(p[0])
                before, after = cols // LANES, (keys.shape[0] - cols - k) // LANES
                ps.append(jnp.concatenate([none] * before + p + [none] * after, axis=1))
                ts.append(t)
                rows, cols = rows + n, cols + k
            ones = jnp.where(iota(keys.shape, 1) < HD, jnp.ones_like(keys), keys)
            o = jnp.dot(jnp.concatenate(ps, axis=0), ones, preferred_element_type=F32)
            rows = 0
            for part, t in zip(tile, ts):
                end = rows + part[0].shape[0]
                done.append((part[3], o[rows:end], jnp.broadcast_to(t, (end - rows, LANES))))
                rows = end
        for places, o, t in done:
            first_row = 0
            for sums, tops, at in places:
                shape = sums[at].shape
                rows = slice(first_row, first_row + math.prod(shape[:-1]))
                sums[at] = o[rows].reshape(shape)
                tops[at] = t[rows].reshape(shape)
                first_row = rows.stop

    def pairs(tiles):
        return [tiles[n : n + 2] for n in range(0, len(tiles), 2)]

    every = slice(None)

    def block(h):
        return kv[:, own0 + h].reshape(BACK, LANES)

    def tile1(h):
        return (
            q2[:, h].reshape(BACK, LANES), jnp.concatenate([block(h - 1), block(h)], axis=0),
            jnp.where(missing, FAR, b1_ref[...]) if h == 0 else b1_ref[...],
            ((acc1, top1, (every, h)),),
        )

    def tile4(c, n):
        blocks = slice(4 * n, 4 * n + 4)
        return (
            q2[c, blocks].reshape(BACK, LANES),
            kv[c, own0 + 4 * n - 4 : own0 + 4 * n + 4].reshape(2 * BACK, LANES),
            b4_ref[...], ((acc4, top4, (c, blocks)),),
        )

    def tile4_first(c, alone):
        keys = kv[c, own0 : own0 + 4].reshape(BACK, LANES)
        b = b4_ref[:, BACK:]
        if alone:
            keys = jnp.concatenate([keys, keys], axis=0)
            b = jnp.concatenate([jnp.full_like(b, FAR), b], axis=1)
        return (q2[c, :4].reshape(BACK, LANES), keys, b, ((acc4, top4, (c, slice(0, 4))),))

    def tile4_old(c):
        return (
            qbf[:4].reshape(BACK, LANES).astype(BF16),
            kv[c, own0 + nq - 4 : own0 + nq].reshape(BACK, LANES),
            b4_ref[:, :BACK], ((accb4, topb4, (every,)),),
        )

    def tile16(c, i, olds):
        rows = slice(8 * i, 8 * i + 8)
        q = q2f[c, :, rows].reshape(BACK, LANES).astype(BF16)
        b = b16_ref[:, BACK:]
        places = ((acc16, top16, (c, every, rows)),)
        if olds:
            old = qbf[:olds, rows].reshape(-1, LANES).astype(BF16)
            q = jnp.concatenate([q, old], axis=0)
            b = jnp.concatenate([b, b16_ref[: old.shape[0], :BACK]], axis=0)
            places = (*places, (accb, topb, (slice(0, olds), rows)))
        return (q, kvf[:, rows].reshape(BACK, LANES).astype(BF16), b, places)

    def tilex(c, i):
        rows = slice(16 * i, 16 * i + 16)
        return (
            q2[c, nh:, rows].reshape(BACK, LANES), kv[c, :nh, rows].reshape(BACK, LANES),
            bx_ref[...], ((accx, topx, (c, every, rows)),),
        )

    each = range(PIECE // 8)
    half = PIECE // 2
    eight = BACK // half
    lane_h = iota((eight, half, LANES), 2)
    low_h = lane_h < HD
    flat = (BACK, LANES)

    def rounded(x):
        return x.astype(BF16).astype(F32)

    def send_old(c, olds):
        t4, t16 = topb4[...], topb[:4]
        t = jnp.maximum(t4, t16)
        accb[:4] = accb[:4] * jnp.exp(t16 - t) + accb4[...] * jnp.exp(t4 - t)
        topb[:4] = t
        stats = jnp.zeros((STATS, LANES), F32)
        for g in range(olds // eight):
            at = slice(g * eight, (g + 1) * eight)
            t = topb[at]
            mark = rounded(t)
            a = accb[at] * jnp.exp(t - mark)
            z = pltpu.roll(a, HD, 2)
            lo, hi = a[:, :half], a[:, half:]
            ob[c, STATS + g * BACK : STATS + (g + 1) * BACK] = (
                jnp.where(low_h, z[:, :half], hi).astype(BF16).reshape(flat)
            )
            columns = mark[:, half:]
            columns = jnp.where(lane_h == 0, mark[:, :half], columns)
            columns = jnp.where(lane_h == 2, rounded(lo), columns)
            columns = jnp.where(lane_h == 3, rounded(hi), columns)
            columns = jnp.where(lane_h == 4, lo - rounded(lo), columns)
            columns = jnp.where(lane_h == 5, hi - rounded(hi), columns)
            pick = (iota((STATS, LANES), 0) - 8 * g == iota((STATS, LANES), 1)) & (
                iota((STATS, LANES), 1) < 6
            )
            stats = stats + lax.dot_general(
                jnp.where(pick, 1.0, 0.0).astype(BF16), columns.astype(BF16).reshape(flat), NT,
                preferred_element_type=F32,
            )
        ob[c, :STATS] = stats.astype(BF16)
        copy_o(c, olds).start()

    def old_rows(olds):
        return slice(0, STATS + olds * half)

    def copy_o(c, olds):
        at = old_rows(olds)
        return remote(ob.at[c, at], oin.at[c, at], s_o, r_o.at[c], target(sp + G, tp))

    def blend(c):
        t4, t16 = top4[c], top16[c]
        t = jnp.maximum(t4, t16)
        acc16[c] = acc4[c] * jnp.exp(t4 - t) + acc16[c] * jnp.exp(t16 - t)
        top16[c] = t

    missing = jnp.logical_and(col < BACK, group == 0)

    @pl.when(jnp.logical_not(has_prev))
    def _():
        kv[:, own0 - 1] = jnp.zeros((CHUNKS, PIECE, LANES), BF16)

    with scope("h_chunks"):
        @pl.loop(0, CHUNKS)
        def _(c):
            drain(qr.at[c, : G - 1], r_q.at[c])
            drain(kv.at[c, own0 : own0 + halves * (G - 1)], r_kv.at[c])
            kvf[...] = kv[c, own0:].astype(F32)
            pl.when(c == 1)(w_away.start)


            def serve(olds):
                if olds:
                    drain(qb.at[c, : olds // halves], r_qb.at[c])
                    unpack(qb, c, olds // halves, qbf)
                unpack(qr, c, G, q2f.at[c], q2)
                four = [tile4_old(c), tile4_first(c, False)] if olds else [tile4_first(c, True)]
                run(
                    [*pairs([tile16(c, i, olds) for i in each]), four]
                    + [[tile4(c, n)] for n in range(1, nq // 4)]
                )
                if olds:
                    send_old(c, olds)
                blend(c)

            @pl.when(jnp.logical_and(has_next, lower))
            def _():
                serve(nh)

            @pl.when(jnp.logical_and(has_next, upper))
            def _():
                serve(nq)

            @pl.when(jnp.logical_not(has_next))
            def _():
                serve(0)


    with scope("i_t1"):
        takes = jnp.logical_and(has_prev, lower)
        ones_tiles = range(nq)

        @pl.when(takes)
        def _():
            drain(kv.at[:, :own0], r_x)
            run(
                [[tile1(h)] for h in ones_tiles]
                + [[tilex(c, i) for i in range(PIECE // 16)] for c in range(CHUNKS)]
            )

        @pl.when(jnp.logical_and(has_prev, upper))
        def _():
            drain(kv.at[:, own0 - 1], r_x)

        @pl.when(jnp.logical_not(takes))
        def _():
            run([[tile1(h)] for h in ones_tiles])

    eye = jnp.where(iota(flat, 0) == iota(flat, 1), 1.0, 0.0).astype(BF16)
    top_rows = iota(flat, 0) < HD

    def merge(c, g, extra=False):
        at = slice(g * eight, (g + 1) * eight)
        parts = [(acc1[c, at], top1[c, at]), (acc16[c, at], top16[c, at])]
        if extra:
            parts.append((accx[c], topx[c]))
        t = functools.reduce(jnp.maximum, [part[1] for part in parts])
        a = sum(part[0] * jnp.exp(part[1] - t) for part in parts)
        z = pltpu.roll(a, HD, 2)
        return (
            jnp.where(low_h, z[:, :half], a[:, half:]),
            jnp.where(low_h, a[:, :half], z[:, half:]),
            jnp.where(low_h, t[:, :half], t[:, half:]),
        )

    def finish(c, g, num, den):
        rs[c, g * eight : (g + 1) * eight] = (num / den).astype(BF16).reshape(eight, half, LANES)

    def finish_old(c, g):
        stats = oin[c, :STATS].astype(F32)

        def spread(j):
            at = 8 * g + j
            both = jnp.where(
                top_rows,
                jnp.broadcast_to(stats[at : at + 1], flat),
                jnp.broadcast_to(stats[at + 1 : at + 2], flat),
            )
            return lax.dot_general(eye, both.astype(BF16), NT, preferred_element_type=F32)

        t = pt[c, g]
        t_old = spread(0)
        t_new = jnp.maximum(t, t_old)
        mine = jnp.exp(t - t_new)
        theirs = jnp.exp(t_old - t_new)
        old = oin[c, STATS + g * BACK : STATS + (g + 1) * BACK].astype(F32)
        finish(
            c, g, pn[c, g] * mine + old * theirs,
            pd[c, g] * mine + (spread(2) + spread(4)) * theirs,
        )

    def copy_ret(c, n):
        return remote(
            rs.at[c, n], rr.at[c, head], s_ret, r_ret,
            target(base + n // tp_count, lax.rem(n, tp_count)),
        )

    def give(c, g):
        for o in quad:
            dest = g * hb + lax.rem(mate(o), hb)
            copy_ret(c, dest * tp_count + tp_count - 1 - tp).start()
            if o:
                copy_ret(c, dest * tp_count + tp).start()
            else:
                @pl.when(dest != me)
                def _():
                    copy_ret(c, dest * tp_count + tp).start()

    groups = range(nq // eight)

    def close(olds, late):
        for c in range(CHUNKS):
            for g in late:
                num, den, t = merge(c, g)
                pn[c, g] = num.reshape(flat)
                pd[c, g] = den.reshape(flat)
                pt[c, g] = t.reshape(flat)

        @pl.loop(0, CHUNKS)
        def _(c):
            drain(oin.at[c, old_rows(olds)], r_o.at[c])
            for g in late:
                finish_old(c, g)
            for g in late:
                give(c, g)

    with scope("o_finish"):
        @pl.when(jnp.logical_and(has_prev, lower))
        def _():
            for c in range(CHUNKS):
                finish(c, 1, *merge(c, 1, True)[:2])
            for c in range(CHUNKS):
                give(c, 1)
            close(nh, (0,))

        @pl.when(jnp.logical_and(has_prev, upper))
        def _():
            close(nq, (0, 1))

        @pl.when(jnp.logical_not(has_prev))
        def _():
            for c in range(CHUNKS):
                for g in groups:
                    finish(c, g, *merge(c, g)[:2])
            for c in range(CHUNKS):
                for g in groups:
                    give(c, g)

        rr[:, head] = rs[:, seat]

    with scope("q_sendwait"):
        drain(kvs.at[:, : G - 1], s_kv)
        drain(qs.at[:, : G - 1], s_q)

        @pl.when(jnp.logical_and(has_prev, lower))
        def _():
            drain(qs, s_qb)

        @pl.when(jnp.logical_and(has_prev, upper))
        def _():
            drain(qs.at[:, :hb], s_qb)

        @pl.when(jnp.logical_and(has_next, lower))
        def _():
            drain(ob.at[:, old_rows(nh)], s_o)

        @pl.when(jnp.logical_and(has_next, upper))
        def _():
            drain(ob, s_o)
            drain(kvs.at[:, :hb], s_x)

        @pl.when(jnp.logical_and(has_next, me == G - 1))
        def _():
            drain(kvs.at[:, :hb, halves - 1], s_y)

        w_local.wait()
        w_away.wait_send()
        pltpu.make_async_remote_copy(
            src_ref=w_ref, dst_ref=wbuf.at[tp_count - 1 - tp],
            send_sem=w_sem.at[1], recv_sem=w_sem.at[2],
            device_id=target(sp, tp_count - 1 - tp), device_id_type=pl.DeviceIdType.MESH,
        ).wait_recv()

    with scope("s_retwait"):
        drain(rr.at[:, : seats - 1], r_ret)

    low_s = iota((half, LANES), 1) < HD
    with scope("t_mix"):
        for m in range(seats // 2):
            x0 = rr[:, 2 * m].astype(F32)
            x1 = rr[:, 2 * m + 1].astype(F32)
            y0 = pltpu.roll(x0, HD, 2)
            y1 = pltpu.roll(x1, HD, 2)
            pair = jnp.concatenate(
                [jnp.where(low_s[None], x0, y1), jnp.where(low_s[None], y0, x1)], axis=1
            ).astype(BF16).reshape(BACK, LANES)
            mx[:, m * LANES : (m + 1) * LANES] = jnp.dot(
                back, pair, preferred_element_type=F32
            ).astype(BF16)

    width = wbuf.shape[1]
    step = out_ref.shape[1]

    with scope("u_proj"):
        @pl.loop(0, out_ref.shape[1] // step)
        def _(c):
            cols = pl.ds(pl.multiple_of(c * step, step), step)
            total = jnp.dot(mx[:, :width], wbuf[0, :, cols], preferred_element_type=F32)
            total = total + jnp.dot(mx[:, width:], wbuf[1, :, cols], preferred_element_type=F32)
            out_ref[:, cols] = total.astype(BF16)

    with scope("v_end"):
        drain(rs.at[:, : seats - 1], s_ret)


def per_device(sp_count, tp_count, query_rows, key_rows, value_rows, out_weight):
    tok = query_rows.shape[0]
    G = query_rows.shape[1] // HD
    halves = tok // BACK
    ngroups = sp_count // G
    assert tok == 2 * BACK and tp_count == 2 and sp_count % G == 0
    assert G & (G - 1) == 0
    assert G * tok == 16 * BACK
    inverse = np.power(THETA, -np.arange(HD // 2) / (HD // 2))
    inverse = np.tile(inverse, LANES // (HD // 2))[None, :]
    local = np.arange(tok)[:, None] * inverse
    cosb = jnp.asarray(np.cos(local), F32)
    sinb = jnp.asarray(np.sin(local), F32)
    inv = jnp.asarray(np.tile(inverse, (8, 1)), F32)
    seats = G * tp_count
    nq = G * halves
    vmem = pl.BlockSpec(memory_space=pltpu.VMEM)
    dma = pltpu.SemaphoreType.DMA
    return pl.pallas_call(
        functools.partial(kernel, G, ngroups, tp_count),
        out_shape=pltpu.VMEM((tok // tp_count, out_weight.shape[1]), BF16),
        in_specs=[pl.BlockSpec(memory_space=pl.ANY)] * 7,
        out_specs=vmem,
        scratch_shapes=[
            pltpu.VMEM(query_rows.shape, BF16),
            pltpu.VMEM(query_rows.shape, BF16),
            pltpu.VMEM(query_rows.shape, BF16),
            pltpu.VMEM(cosb.shape, F32),
            pltpu.VMEM(sinb.shape, F32),
            pltpu.VMEM(inv.shape, F32),
            pltpu.VMEM((CHUNKS, G, PIECE, LANES), BF16),
            pltpu.VMEM((CHUNKS, G, halves, PIECE, LANES), BF16),
            pltpu.VMEM((CHUNKS, G, PIECE, LANES), BF16),
            pltpu.VMEM((CHUNKS, nq + nq // 2, PIECE, LANES), BF16),
            pltpu.VMEM((nq, PIECE, LANES), F32),
            pltpu.VMEM((CHUNKS, nq, PIECE, LANES), BF16),
            *[pltpu.VMEM((CHUNKS, nq, PIECE, LANES), F32)] * 7,
            *[pltpu.VMEM((CHUNKS, nq // 2, PIECE, LANES), F32)] * 2,
            pltpu.VMEM((CHUNKS, G, PIECE, LANES), BF16),
            *[pltpu.VMEM((nq, PIECE, LANES), F32)] * 3,
            *[pltpu.VMEM((4, PIECE, LANES), F32)] * 2,
            *[pltpu.VMEM((CHUNKS, STATS + nq * PIECE // 2, LANES), BF16)] * 2,
            *[pltpu.VMEM((CHUNKS, nq * PIECE // (2 * BACK), BACK, LANES), F32)] * 3,
            pltpu.VMEM((BACK, 2 * BACK), F32),
            pltpu.VMEM((BACK, 2 * BACK), F32),
            pltpu.VMEM((BACK, 2 * BACK), F32),
            pltpu.VMEM((BACK, BACK), F32),
            pltpu.VMEM((tp_count,) + out_weight.shape, BF16),
            pltpu.VMEM((CHUNKS, seats, PIECE // 2, LANES), BF16),
            pltpu.VMEM((CHUNKS, seats, PIECE // 2, LANES), BF16),
            pltpu.VMEM((BACK, seats * HD), BF16),
            dma, dma, dma, dma, dma, dma, dma,
            dma((CHUNKS,)), dma((CHUNKS,)), dma((CHUNKS,)), dma, dma((CHUNKS,)), dma,
            dma((3,)), dma((6,)),
        ],
        compiler_params=pltpu.CompilerParams(
            collective_id=0, has_side_effects=True, vmem_limit_bytes=63 * 1024 * 1024
        ),
    )(query_rows, key_rows, value_rows, cosb, sinb, inv, out_weight)


def solution(mesh):
    return jax.shard_map(
        functools.partial(per_device, mesh.shape["sp"], mesh.shape["tp"]),
        mesh=mesh,
        in_specs=(P("sp", "tp"), P("sp", "tp"), P("sp", "tp"), P("tp", None)),
        out_specs=P(("sp", "tp"), None),
        check_vma=False,
    )
```

```python
import functools
import math

import jax
import jax.numpy as jnp
import numpy as np
from jax import lax
from jax.experimental import pallas as pl
from jax.experimental.pallas import tpu as pltpu
from jax.sharding import PartitionSpec as P

HD = 64
BACK = 128
THETA = 500000.0
FAR = -1e30
F32 = jnp.float32
BF16 = jnp.bfloat16
LANES = 2 * HD
CHUNKS = 4
PIECE = BACK // CHUNKS
STATS = 16
NT = (((1,), (1,)), ((), ()))


def place(p):
    return ((p & 7) << 4) + (((p >> 3) & 3) << 2) + (p >> 5)


def iota(shape, axis):
    return lax.broadcasted_iota(jnp.int32, shape, axis)


def kernel(
    G, ngroups, tp_count,
    q_hbm, k_hbm, v_hbm, cosb_hbm, sinb_hbm, inv_hbm, w_ref, out_ref,
    q_ref, k_ref, v_ref, cosb_ref, sinb_ref, inv_ref, qs, kvs, qr, kv, kvf, q2, q2f,
    acc1, top1, acc4, top4, acc16, top16, accx, topx, qb, qbf, accb, topb, accb4, topb4, ob, oin, pn, pd, pt, b1_ref, b4_ref, b16_ref, bx_ref, wbuf, rs, rr, mx,
    s_kv, s_q, s_qb, s_x, s_y, s_o, s_ret, r_kv, r_q, r_qb, r_x, r_o, r_ret, w_sem, in_sem,
):
    loads = [
        pltpu.make_async_copy(source, dest, in_sem.at[n])
        for n, (source, dest) in enumerate((
            (inv_hbm, inv_ref), (cosb_hbm, cosb_ref), (sinb_hbm, sinb_ref),
            (k_hbm, k_ref), (v_hbm, v_ref), (q_hbm, q_ref),
        ))
    ]
    for load in loads:
        load.start()
    sp = lax.axis_index("sp")
    tp = lax.axis_index("tp")
    group = sp // G
    me = sp - group * G
    base = group * G
    has_prev = group > 0
    has_next = group < ngroups - 1
    seat = me * tp_count + tp
    seats = G * tp_count
    head = tp * G + me
    tok = q_ref.shape[0]
    halves = tok // BACK
    nq = G * halves
    hb = G // 2
    nh = nq // 2
    own0 = nh
    lower = me < hb
    upper = me >= hb

    def target(s, t):
        return {"sp": s, "tp": t}

    barrier = pltpu.get_barrier_semaphore()
    for o in range(1, seats):
        n = lax.rem(seat + o, seats)
        pl.semaphore_signal(
            barrier, inc=1, device_id=target(base + n // tp_count, lax.rem(n, tp_count)),
            device_id_type=pl.DeviceIdType.MESH,
        )

    @pl.when(has_prev)
    def _():
        for o in range(G):
            pl.semaphore_signal(
                barrier, inc=1, device_id=target(base - G + o, tp),
                device_id_type=pl.DeviceIdType.MESH,
            )

    @pl.when(has_next)
    def _():
        for o in range(G):
            pl.semaphore_signal(
                barrier, inc=1, device_id=target(base + G + o, tp),
                device_id_type=pl.DeviceIdType.MESH,
            )

    w_local = pltpu.make_async_copy(w_ref, wbuf.at[tp], w_sem.at[0])
    w_local.start()

    def stride4(n):
        w = n & 31
        return ((n >> 5) << 5) + ((w & 7) << 2) + (w >> 3)

    def masked(distance):
        return jnp.where((distance >= 0) & (distance <= BACK), 0.0, FAR)

    row = iota((BACK, 2 * BACK), 0)
    col = iota((BACK, 2 * BACK), 1)
    b1_ref[...] = masked(place(row) + BACK - place(col & (BACK - 1)) - ((col >> 7) << 7))
    b4_ref[...] = masked(stride4(row) + BACK - stride4(col))
    b16_ref[...] = masked(row + BACK - col)

    def stride16(n):
        return ((n >> 4) << 3) + (n & 7)

    xrow = iota((BACK, BACK), 0)
    xcol = iota((BACK, BACK), 1)
    same = ((xrow ^ xcol) & 8) == 0
    bx_ref[...] = jnp.where(same, masked(stride16(xrow) + BACK - stride16(xcol)), FAR)

    scope = jax.named_scope
    with scope("a_loads"):
        for load in loads:
            load.wait()

    lane = iota((BACK, LANES), 1)
    low = lane < HD
    lane_t = iota((tok, LANES), 1)
    first = (lane_t & (HD - 1)) < HD // 2
    angle = inv_ref[...] * (sp * tok).astype(F32)
    ca = jnp.cos(angle)[:1]
    sa = jnp.sin(angle)[:1]
    cos = ca * cosb_ref[...] - sa * sinb_ref[...]
    sin = sa * cosb_ref[...] + ca * sinb_ref[...]
    sin = jnp.where(first, -sin, sin)
    swizzle = jnp.where(place(iota((BACK, BACK), 0)) == iota((BACK, BACK), 1), 1.0, 0.0).astype(BF16)
    back = jnp.where(place(iota((BACK, BACK), 1)) == iota((BACK, BACK), 0), 1.0, 0.0).astype(BF16)

    def turn(ref, cols):
        x = ref[:, cols].astype(F32)
        other = jnp.where(first, pltpu.roll(x, LANES - HD // 2, 1), pltpu.roll(x, HD // 2, 1))
        return (x * cos + other * sin).astype(BF16)

    def sw(x):
        return jnp.dot(swizzle, x, preferred_element_type=F32)

    def cut(x):
        return x.astype(BF16).reshape(CHUNKS, PIECE, LANES)

    with scope("c_turn"):
        for m in range(G // 2):
            cols = slice(m * LANES, (m + 1) * LANES)
            tq = turn(q_ref, cols)
            tk = turn(k_ref, cols)
            tv = v_ref[:, cols]
            q_a = sw(tq[:BACK]) * (1.0 / math.sqrt(HD))
            q_b = sw(tq[BACK:]) * (1.0 / math.sqrt(HD))
            qs[:, 2 * m] = cut(jnp.where(low, q_a, pltpu.roll(q_b, HD, 1)))
            qs[:, 2 * m + 1] = cut(jnp.where(low, pltpu.roll(q_a, HD, 1), q_b))
            for e in range(halves):
                ks = sw(tk[e * BACK : (e + 1) * BACK])
                vs = sw(tv[e * BACK : (e + 1) * BACK])
                kvs[:, 2 * m, e] = cut(jnp.where(low, ks, pltpu.roll(vs, HD, 1)))
                kvs[:, 2 * m + 1, e] = cut(jnp.where(low, pltpu.roll(ks, HD, 1), vs))

    with scope("d_barrier"):
        pl.semaphore_wait(
            barrier, seats - 1 + jnp.where(has_prev, G, 0) + jnp.where(has_next, G, 0)
        )

    def remote(source, dest, send, recv, device):
        return pltpu.make_async_remote_copy(
            src_ref=source, dst_ref=dest, send_sem=send, recv_sem=recv,
            device_id=device, device_id_type=pl.DeviceIdType.MESH,
        )

    def drain(ref, sem):
        pltpu.make_async_copy(ref, ref, sem).wait()

    def copy_kv(c, dest):
        return remote(
            kvs.at[c, dest], kv.at[c, pl.ds(own0 + halves * me, halves)],
            s_kv, r_kv.at[c], target(base + dest, tp),
        )

    def copy_q(c, dest):
        return remote(qs.at[c, dest], qr.at[c, me], s_q, r_q.at[c], target(base + dest, tp))

    def copy_qb(c, dest):
        return remote(
            qs.at[c, dest], qb.at[c, me], s_qb, r_qb.at[c], target(base - G + dest, tp)
        )

    def copy_y(c, dest):
        return remote(
            kvs.at[c, dest, halves - 1], kv.at[c, own0 - 1], s_y, r_x, target(base + G + dest, tp)
        )

    def copy_x(c, dest):
        return remote(
            kvs.at[c, dest], kv.at[c, pl.ds(halves * (me - hb), halves)],
            s_x, r_x, target(base + G + dest, tp),
        )

    w_away = pltpu.make_async_remote_copy(
        src_ref=w_ref, dst_ref=wbuf.at[tp], send_sem=w_sem.at[1], recv_sem=w_sem.at[2],
        device_id=target(sp, tp_count - 1 - tp), device_id_type=pl.DeviceIdType.MESH,
    )

    bits = [1 << n for n in range(G.bit_length() - 1)]
    far = sorted(range(1, G), key=lambda o: -o.bit_count())

    quad = [o for o in far if o < hb] + [0]

    def mate(o):
        return sum((((me // b + o // b) % 2) * b for b in bits), 0)

    def send_back(c):
        @pl.when(jnp.logical_and(has_prev, lower))
        def _():
            for o in [*far, 0]:
                copy_qb(c, mate(o)).start()

        @pl.when(jnp.logical_and(has_prev, upper))
        def _():
            for o in quad:
                copy_qb(c, hb + lax.rem(mate(o), hb)).start()

    with scope("e_issue"):
        @pl.when(jnp.logical_and(has_next, upper))
        def _():
            for c in range(CHUNKS):
                for o in quad:
                    copy_x(c, lax.rem(mate(o), hb)).start()

        @pl.when(jnp.logical_and(has_next, me == G - 1))
        def _():
            for c in range(CHUNKS):
                for o in quad:
                    copy_y(c, hb + lax.rem(mate(o), hb)).start()

        for c in range(CHUNKS):
            send_back(c)
            for o in far:
                copy_q(c, mate(o)).start()
                copy_kv(c, mate(o)).start()

    for c in range(CHUNKS):
        kv[c, pl.ds(own0 + halves * me, halves)] = kvs[c, me]
        qr[c, me] = qs[c, me]

    low_p = low[:PIECE]

    def unpack(ref, c, sources, wide, narrow=None):
        for s in range(sources):
            x = ref[c, s].astype(F32)
            a = jnp.where(low_p, x, 0.0)
            b = jnp.where(low_p, pltpu.roll(x, HD, 1), 0.0)
            wide[2 * s] = a
            wide[2 * s + 1] = b
            if narrow is not None:
                narrow[c, 2 * s] = a.astype(BF16)
                narrow[c, 2 * s + 1] = b.astype(BF16)

    def run(tiles):
        done = []
        for tile in tiles:
            q = jnp.concatenate([part[0] for part in tile], axis=0)
            keys = jnp.concatenate([part[1] for part in tile], axis=0)
            s = lax.dot_general(q, keys, NT, preferred_element_type=F32)
            rows, cols, ps, ts = 0, 0, [], []
            for part in tile:
                n, k = part[0].shape[0], part[1].shape[0]
                mine = s[rows : rows + n, cols : cols + k] + part[2]
                t = jnp.max(mine, axis=1, keepdims=True)
                p = [
                    jnp.exp(mine[:, a : a + LANES] - t).astype(BF16) for a in range(0, k, LANES)
                ]
                none = jnp.zeros_like(p[0])
                before, after = cols // LANES, (keys.shape[0] - cols - k) // LANES
                ps.append(jnp.concatenate([none] * before + p + [none] * after, axis=1))
                ts.append(t)
                rows, cols = rows + n, cols + k
            ones = jnp.where(iota(keys.shape, 1) < HD, jnp.ones_like(keys), keys)
            o = jnp.dot(jnp.concatenate(ps, axis=0), ones, preferred_element_type=F32)
            rows = 0
            for part, t in zip(tile, ts):
                end = rows + part[0].shape[0]
                done.append((part[3], o[rows:end], jnp.broadcast_to(t, (end - rows, LANES))))
                rows = end
        for places, o, t in done:
            first_row = 0
            for sums, tops, at in places:
                shape = sums[at].shape
                rows = slice(first_row, first_row + math.prod(shape[:-1]))
                sums[at] = o[rows].reshape(shape)
                tops[at] = t[rows].reshape(shape)
                first_row = rows.stop

    def pairs(tiles):
        return [tiles[n : n + 2] for n in range(0, len(tiles), 2)]

    every = slice(None)

    def block(h):
        return kv[:, own0 + h].reshape(BACK, LANES)

    def tile1(h):
        return (
            q2[:, h].reshape(BACK, LANES), jnp.concatenate([block(h - 1), block(h)], axis=0),
            jnp.where(missing, FAR, b1_ref[...]) if h == 0 else b1_ref[...],
            ((acc1, top1, (every, h)),),
        )

    def tile4(c, n):
        blocks = slice(4 * n, 4 * n + 4)
        return (
            q2[c, blocks].reshape(BACK, LANES),
            kv[c, own0 + 4 * n - 4 : own0 + 4 * n + 4].reshape(2 * BACK, LANES),
            b4_ref[...], ((acc4, top4, (c, blocks)),),
        )

    def tile4_first(c, alone):
        keys = kv[c, own0 : own0 + 4].reshape(BACK, LANES)
        b = b4_ref[:, BACK:]
        if alone:
            keys = jnp.concatenate([keys, keys], axis=0)
            b = jnp.concatenate([jnp.full_like(b, FAR), b], axis=1)
        return (q2[c, :4].reshape(BACK, LANES), keys, b, ((acc4, top4, (c, slice(0, 4))),))

    def tile4_old(c):
        return (
            qbf[:4].reshape(BACK, LANES).astype(BF16),
            kv[c, own0 + nq - 4 : own0 + nq].reshape(BACK, LANES),
            b4_ref[:, :BACK], ((accb4, topb4, (every,)),),
        )

    def tile16(c, i, olds):
        rows = slice(8 * i, 8 * i + 8)
        q = q2f[c, :, rows].reshape(BACK, LANES).astype(BF16)
        b = b16_ref[:, BACK:]
        places = ((acc16, top16, (c, every, rows)),)
        if olds:
            old = qbf[:olds, rows].reshape(-1, LANES).astype(BF16)
            q = jnp.concatenate([q, old], axis=0)
            b = jnp.concatenate([b, b16_ref[: old.shape[0], :BACK]], axis=0)
            places = (*places, (accb, topb, (slice(0, olds), rows)))
        return (q, kvf[:, rows].reshape(BACK, LANES).astype(BF16), b, places)

    def tilex(c, i):
        rows = slice(16 * i, 16 * i + 16)
        return (
            q2[c, nh:, rows].reshape(BACK, LANES), kv[c, :nh, rows].reshape(BACK, LANES),
            bx_ref[...], ((accx, topx, (c, every, rows)),),
        )

    each = range(PIECE // 8)
    half = PIECE // 2
    eight = BACK // half
    lane_h = iota((eight, half, LANES), 2)
    low_h = lane_h < HD
    flat = (BACK, LANES)

    def rounded(x):
        return x.astype(BF16).astype(F32)

    def send_old(c, olds):
        t4, t16 = topb4[...], topb[:4]
        t = jnp.maximum(t4, t16)
        accb[:4] = accb[:4] * jnp.exp(t16 - t) + accb4[...] * jnp.exp(t4 - t)
        topb[:4] = t
        stats = jnp.zeros((STATS, LANES), F32)
        for g in range(olds // eight):
            at = slice(g * eight, (g + 1) * eight)
            t = topb[at]
            mark = rounded(t)
            a = accb[at] * jnp.exp(t - mark)
            z = pltpu.roll(a, HD, 2)
            lo, hi = a[:, :half], a[:, half:]
            ob[c, STATS + g * BACK : STATS + (g + 1) * BACK] = (
                jnp.where(low_h, z[:, :half], hi).astype(BF16).reshape(flat)
            )
            columns = mark[:, half:]
            columns = jnp.where(lane_h == 0, mark[:, :half], columns)
            columns = jnp.where(lane_h == 2, rounded(lo), columns)
            columns = jnp.where(lane_h == 3, rounded(hi), columns)
            columns = jnp.where(lane_h == 4, lo - rounded(lo), columns)
            columns = jnp.where(lane_h == 5, hi - rounded(hi), columns)
            pick = (iota((STATS, LANES), 0) - 8 * g == iota((STATS, LANES), 1)) & (
                iota((STATS, LANES), 1) < 6
            )
            stats = stats + lax.dot_general(
                jnp.where(pick, 1.0, 0.0).astype(BF16), columns.astype(BF16).reshape(flat), NT,
                preferred_element_type=F32,
            )
        ob[c, :STATS] = stats.astype(BF16)
        copy_o(c, olds).start()

    def old_rows(olds):
        return slice(0, STATS + olds * half)

    def copy_o(c, olds):
        at = old_rows(olds)
        return remote(ob.at[c, at], oin.at[c, at], s_o, r_o.at[c], target(sp + G, tp))

    def blend(c):
        t4, t16 = top4[c], top16[c]
        t = jnp.maximum(t4, t16)
        acc16[c] = acc4[c] * jnp.exp(t4 - t) + acc16[c] * jnp.exp(t16 - t)
        top16[c] = t

    missing = jnp.logical_and(col < BACK, group == 0)

    @pl.when(jnp.logical_not(has_prev))
    def _():
        kv[:, own0 - 1] = jnp.zeros((CHUNKS, PIECE, LANES), BF16)

    with scope("h_chunks"):
        @pl.loop(0, CHUNKS)
        def _(c):
            drain(qr.at[c, : G - 1], r_q.at[c])
            drain(kv.at[c, own0 : own0 + halves * (G - 1)], r_kv.at[c])
            kvf[...] = kv[c, own0:].astype(F32)
            pl.when(c == 1)(w_away.start)


            def serve(olds):
                if olds:
                    drain(qb.at[c, : olds // halves], r_qb.at[c])
                    unpack(qb, c, olds // halves, qbf)
                unpack(qr, c, G, q2f.at[c], q2)
                four = [tile4_old(c), tile4_first(c, False)] if olds else [tile4_first(c, True)]
                run(
                    [*pairs([tile16(c, i, olds) for i in each]), four]
                    + [[tile4(c, n)] for n in range(1, nq // 4)]
                )
                if olds:
                    send_old(c, olds)
                blend(c)

            @pl.when(jnp.logical_and(has_next, lower))
            def _():
                serve(nh)

            @pl.when(jnp.logical_and(has_next, upper))
            def _():
                serve(nq)

            @pl.when(jnp.logical_not(has_next))
            def _():
                serve(0)


    with scope("i_t1"):
        takes = jnp.logical_and(has_prev, lower)
        ones_tiles = range(nq)

        @pl.when(takes)
        def _():
            drain(kv.at[:, :own0], r_x)
            run(
                [[tile1(h)] for h in ones_tiles]
                + [[tilex(c, i) for i in range(PIECE // 16)] for c in range(CHUNKS)]
            )

        @pl.when(jnp.logical_and(has_prev, upper))
        def _():
            drain(kv.at[:, own0 - 1], r_x)

        @pl.when(jnp.logical_not(takes))
        def _():
            run([[tile1(h)] for h in ones_tiles])

    eye = jnp.where(iota(flat, 0) == iota(flat, 1), 1.0, 0.0).astype(BF16)
    top_rows = iota(flat, 0) < HD

    def merge(c, g, extra=False):
        at = slice(g * eight, (g + 1) * eight)
        parts = [(acc1[c, at], top1[c, at]), (acc16[c, at], top16[c, at])]
        if extra:
            parts.append((accx[c], topx[c]))
        t = functools.reduce(jnp.maximum, [part[1] for part in parts])
        a = sum(part[0] * jnp.exp(part[1] - t) for part in parts)
        z = pltpu.roll(a, HD, 2)
        return (
            jnp.where(low_h, z[:, :half], a[:, half:]),
            jnp.where(low_h, a[:, :half], z[:, half:]),
            jnp.where(low_h, t[:, :half], t[:, half:]),
        )

    def finish(c, g, num, den):
        rs[c, g * eight : (g + 1) * eight] = (num / den).astype(BF16).reshape(eight, half, LANES)

    def finish_old(c, g):
        stats = oin[c, :STATS].astype(F32)

        def spread(j):
            at = 8 * g + j
            both = jnp.where(
                top_rows,
                jnp.broadcast_to(stats[at : at + 1], flat),
                jnp.broadcast_to(stats[at + 1 : at + 2], flat),
            )
            return lax.dot_general(eye, both.astype(BF16), NT, preferred_element_type=F32)

        t = pt[c, g]
        t_old = spread(0)
        t_new = jnp.maximum(t, t_old)
        mine = jnp.exp(t - t_new)
        theirs = jnp.exp(t_old - t_new)
        old = oin[c, STATS + g * BACK : STATS + (g + 1) * BACK].astype(F32)
        finish(
            c, g, pn[c, g] * mine + old * theirs,
            pd[c, g] * mine + (spread(2) + spread(4)) * theirs,
        )

    def copy_ret(c, n):
        return remote(
            rs.at[c, n], rr.at[c, head], s_ret, r_ret,
            target(base + n // tp_count, lax.rem(n, tp_count)),
        )

    def give(c, g):
        for o in quad:
            dest = g * hb + lax.rem(mate(o), hb)
            copy_ret(c, dest * tp_count + tp_count - 1 - tp).start()
            if o:
                copy_ret(c, dest * tp_count + tp).start()
            else:
                @pl.when(dest != me)
                def _():
                    copy_ret(c, dest * tp_count + tp).start()

    groups = range(nq // eight)

    def close(olds, late):
        for c in range(CHUNKS):
            for g in late:
                num, den, t = merge(c, g)
                pn[c, g] = num.reshape(flat)
                pd[c, g] = den.reshape(flat)
                pt[c, g] = t.reshape(flat)

        @pl.loop(0, CHUNKS)
        def _(c):
            drain(oin.at[c, old_rows(olds)], r_o.at[c])
            for g in late:
                finish_old(c, g)
            for g in late:
                give(c, g)

    with scope("o_finish"):
        @pl.when(jnp.logical_and(has_prev, lower))
        def _():
            for c in range(CHUNKS):
                finish(c, 1, *merge(c, 1, True)[:2])
            for c in range(CHUNKS):
                give(c, 1)
            close(nh, (0,))

        @pl.when(jnp.logical_and(has_prev, upper))
        def _():
            close(nq, (0, 1))

        @pl.when(jnp.logical_not(has_prev))
        def _():
            for part in (range(CHUNKS // 2), range(CHUNKS // 2, CHUNKS)):
                for c in part:
                    for g in groups:
                        finish(c, g, *merge(c, g)[:2])
                for c in part:
                    for g in groups:
                        give(c, g)

        rr[:, head] = rs[:, seat]

    with scope("q_sendwait"):
        drain(kvs.at[:, : G - 1], s_kv)
        drain(qs.at[:, : G - 1], s_q)

        @pl.when(jnp.logical_and(has_prev, lower))
        def _():
            drain(qs, s_qb)

        @pl.when(jnp.logical_and(has_prev, upper))
        def _():
            drain(qs.at[:, :hb], s_qb)

        @pl.when(jnp.logical_and(has_next, lower))
        def _():
            drain(ob.at[:, old_rows(nh)], s_o)

        @pl.when(jnp.logical_and(has_next, upper))
        def _():
            drain(ob, s_o)
            drain(kvs.at[:, :hb], s_x)

        @pl.when(jnp.logical_and(has_next, me == G - 1))
        def _():
            drain(kvs.at[:, :hb, halves - 1], s_y)

        w_local.wait()
        w_away.wait_send()
        pltpu.make_async_remote_copy(
            src_ref=w_ref, dst_ref=wbuf.at[tp_count - 1 - tp],
            send_sem=w_sem.at[1], recv_sem=w_sem.at[2],
            device_id=target(sp, tp_count - 1 - tp), device_id_type=pl.DeviceIdType.MESH,
        ).wait_recv()

    with scope("s_retwait"):
        drain(rr.at[:, : seats - 1], r_ret)

    low_s = iota((half, LANES), 1) < HD
    with scope("t_mix"):
        for m in range(seats // 2):
            x0 = rr[:, 2 * m].astype(F32)
            x1 = rr[:, 2 * m + 1].astype(F32)
            y0 = pltpu.roll(x0, HD, 2)
            y1 = pltpu.roll(x1, HD, 2)
            pair = jnp.concatenate(
                [jnp.where(low_s[None], x0, y1), jnp.where(low_s[None], y0, x1)], axis=1
            ).astype(BF16).reshape(BACK, LANES)
            mx[:, m * LANES : (m + 1) * LANES] = jnp.dot(
                back, pair, preferred_element_type=F32
            ).astype(BF16)

    width = wbuf.shape[1]
    step = out_ref.shape[1]

    with scope("u_proj"):
        @pl.loop(0, out_ref.shape[1] // step)
        def _(c):
            cols = pl.ds(pl.multiple_of(c * step, step), step)
            total = jnp.dot(mx[:, :width], wbuf[0, :, cols], preferred_element_type=F32)
            total = total + jnp.dot(mx[:, width:], wbuf[1, :, cols], preferred_element_type=F32)
            out_ref[:, cols] = total.astype(BF16)

    with scope("v_end"):
        drain(rs.at[:, : seats - 1], s_ret)


def per_device(sp_count, tp_count, query_rows, key_rows, value_rows, out_weight):
    tok = query_rows.shape[0]
    G = query_rows.shape[1] // HD
    halves = tok // BACK
    ngroups = sp_count // G
    assert tok == 2 * BACK and tp_count == 2 and sp_count % G == 0
    assert G & (G - 1) == 0
    assert G * tok == 16 * BACK
    inverse = np.power(THETA, -np.arange(HD // 2) / (HD // 2))
    inverse = np.tile(inverse, LANES // (HD // 2))[None, :]
    local = np.arange(tok)[:, None] * inverse
    cosb = jnp.asarray(np.cos(local), F32)
    sinb = jnp.asarray(np.sin(local), F32)
    inv = jnp.asarray(np.tile(inverse, (8, 1)), F32)
    seats = G * tp_count
    nq = G * halves
    vmem = pl.BlockSpec(memory_space=pltpu.VMEM)
    dma = pltpu.SemaphoreType.DMA
    return pl.pallas_call(
        functools.partial(kernel, G, ngroups, tp_count),
        out_shape=pltpu.VMEM((tok // tp_count, out_weight.shape[1]), BF16),
        in_specs=[pl.BlockSpec(memory_space=pl.ANY)] * 7,
        out_specs=vmem,
        scratch_shapes=[
            pltpu.VMEM(query_rows.shape, BF16),
            pltpu.VMEM(query_rows.shape, BF16),
            pltpu.VMEM(query_rows.shape, BF16),
            pltpu.VMEM(cosb.shape, F32),
            pltpu.VMEM(sinb.shape, F32),
            pltpu.VMEM(inv.shape, F32),
            pltpu.VMEM((CHUNKS, G, PIECE, LANES), BF16),
            pltpu.VMEM((CHUNKS, G, halves, PIECE, LANES), BF16),
            pltpu.VMEM((CHUNKS, G, PIECE, LANES), BF16),
            pltpu.VMEM((CHUNKS, nq + nq // 2, PIECE, LANES), BF16),
            pltpu.VMEM((nq, PIECE, LANES), F32),
            pltpu.VMEM((CHUNKS, nq, PIECE, LANES), BF16),
            *[pltpu.VMEM((CHUNKS, nq, PIECE, LANES), F32)] * 7,
            *[pltpu.VMEM((CHUNKS, nq // 2, PIECE, LANES), F32)] * 2,
            pltpu.VMEM((CHUNKS, G, PIECE, LANES), BF16),
            *[pltpu.VMEM((nq, PIECE, LANES), F32)] * 3,
            *[pltpu.VMEM((4, PIECE, LANES), F32)] * 2,
            *[pltpu.VMEM((CHUNKS, STATS + nq * PIECE // 2, LANES), BF16)] * 2,
            *[pltpu.VMEM((CHUNKS, nq * PIECE // (2 * BACK), BACK, LANES), F32)] * 3,
            pltpu.VMEM((BACK, 2 * BACK), F32),
            pltpu.VMEM((BACK, 2 * BACK), F32),
            pltpu.VMEM((BACK, 2 * BACK), F32),
            pltpu.VMEM((BACK, BACK), F32),
            pltpu.VMEM((tp_count,) + out_weight.shape, BF16),
            pltpu.VMEM((CHUNKS, seats, PIECE // 2, LANES), BF16),
            pltpu.VMEM((CHUNKS, seats, PIECE // 2, LANES), BF16),
            pltpu.VMEM((BACK, seats * HD), BF16),
            dma, dma, dma, dma, dma, dma, dma,
            dma((CHUNKS,)), dma((CHUNKS,)), dma((CHUNKS,)), dma, dma((CHUNKS,)), dma,
            dma((3,)), dma((6,)),
        ],
        compiler_params=pltpu.CompilerParams(
            collective_id=0, has_side_effects=True, vmem_limit_bytes=63 * 1024 * 1024
        ),
    )(query_rows, key_rows, value_rows, cosb, sinb, inv, out_weight)


def solution(mesh):
    return jax.shard_map(
        functools.partial(per_device, mesh.shape["sp"], mesh.shape["tp"]),
        mesh=mesh,
        in_specs=(P("sp", "tp"), P("sp", "tp"), P("sp", "tp"), P("tp", None)),
        out_specs=P(("sp", "tp"), None),
        check_vma=False,
    )
```
